512 devices in a mesh: grp: 2 (over y), ep: 32 (over z, core), tp: 8 (over x).
Axes of the slice: x: 8, y: 2, z: 16, core: 2. Of those that a mesh axis runs over, the one named last changes fastest.
The devices are a block of a 8x8x16 slice.
Arguments:
- tokens: bfloat16 [4096, 4096], P(('grp', 'ep'), 'tp'), parts along dimension 0, may hold values from -27 to 27
- group_choice: int32 [4096], P(('grp', 'ep')), parts along dimension 0, may hold values from 0 to 3, as said below
- member_choice: int32 [4096, 4], P(('grp', 'ep')), parts along dimension 0, may hold values from 0 to 7, as said below
- group_prob: float32 [4096], P(('grp', 'ep')), parts along dimension 0, may hold values from 0.3 to 1
- member_score: float32 [4096, 4], P(('grp', 'ep')), parts along dimension 0, may hold values from -4 to 4
- norm_gain: float32 [4096], P('tp'), may hold values from 0.1 to 1.9
- w_gate: bfloat16 [32, 4096, 1024], P('ep', 'tp'), may hold values from -0.09375 to 0.09375
- w_up: bfloat16 [32, 4096, 1024], P('ep', 'tp'), may hold values from -0.09375 to 0.09375
- w_down: bfloat16 [32, 1024, 4096], P('ep', None, 'tp'), may hold values from -0.1875 to 0.1875
- final_gain: float32 [4096], P('tp'), may hold values from 0.1 to 1.9
Outputs:
- mixed: bfloat16 [4096, 4096], P(('grp', 'ep'), 'tp'), parts along dimension 0
The draws below stay inside these ranges and needn't reach their ends.
There are 2 independent parts, one for each index of `grp`. The reference program is written for one: setup_inputs(seed, part) draws one part's arguments, and reference() takes and returns one part's arrays. A program takes and returns all parts, laid end to end along the dimension named above; an argument that names none is the same for every part. Nothing has to cross between parts.
Inputs may be any that keep to these rules, and one draw needn't show every extreme that they name: `group_choice`: in each aligned block of 64 tokens every group is chosen by exactly 16 tokens. `member_choice`: each row names 4 different experts of its token's group. In each aligned block of 64 rows no expert (group and member together) is named by more than 16 rows, some expert is named by exactly 16 rows, and one expert is named by exactly 16 rows in every block.
All inputs are finite; a program needn't handle non-finite values.
Results may differ from the reference program's by a relative error of at most 0.017.
Values may be sent and summed in bfloat16 or wider, within the bound.
A program may use at most 64 MiB of HBM per device.

```python
import jax
import jax.numpy as jnp
from jax import lax

D = 4096
FF = 1024
TOK_DEV = 64
EXPERTS = 32
GROUPS = 4
PER_GROUP = 8
TOP = 4
CAP = 16
TOKENS = 2048
N_EP = 32
N_TP = 8


def block_order(block_key):
    return jax.random.permutation(block_key, TOK_DEV)


def routing_draw(key):
    order_keys = jax.random.split(jax.random.fold_in(key, 101), N_EP)
    orderings = jax.vmap(block_order)(order_keys).astype(jnp.int32)
    groups_of = (orderings // CAP).astype(jnp.int32)
    favourite = jax.random.randint(jax.random.fold_in(key, 102), (GROUPS,), 0, PER_GROUP)
    coin_flip = jax.random.randint(jax.random.fold_in(key, 103), (N_EP, GROUPS), 0, 2)
    others = jax.random.randint(jax.random.fold_in(key, 104), (N_EP, GROUPS), 0, PER_GROUP)
    hot_member = jnp.where(coin_flip == 1, favourite[None, :], others)
    hot_member = hot_member.at[:, 0].set(favourite[0])
    token_hot = jnp.take_along_axis(hot_member, groups_of, axis=1)
    member_iota = jnp.arange(PER_GROUP, dtype=jnp.int32)
    raw_scores = jax.random.randint(jax.random.fold_in(key, 105), (N_EP, TOK_DEV, PER_GROUP), 0, 1 << 20)
    ranking = raw_scores * PER_GROUP + member_iota[None, None, :]
    ranking = jnp.where(member_iota[None, None, :] == token_hot[:, :, None], -1, ranking)
    members = jnp.argsort(ranking, axis=2)[:, :, :TOP]
    shuffle_scores = jax.random.randint(jax.random.fold_in(key, 106), (N_EP, TOK_DEV, TOP), 0, 1 << 20)
    shuffle_scores = shuffle_scores * TOP + jnp.arange(TOP, dtype=jnp.int32)[None, None, :]
    members = jnp.take_along_axis(members, jnp.argsort(shuffle_scores, axis=2), axis=2)
    return (groups_of.reshape(TOKENS).astype(jnp.int32), members.reshape(TOKENS, TOP).astype(jnp.int32))


def draw_group_choice(key, part):
    return routing_draw(key)[0]


def draw_member_choice(key, part):
    return routing_draw(key)[1]


def draw_tokens(key, part):
    col_pos = jnp.arange(D, dtype=jnp.float32) / D
    col_jitter = jax.random.uniform(jax.random.fold_in(key, 201), (D,), jnp.float32)
    col_scale = jnp.exp(jnp.log(10.0) * (0.5 * col_pos + 0.5 * col_jitter))
    row_scale = jnp.exp(jax.random.uniform(jax.random.fold_in(key, 202), (TOKENS, 1), jnp.float32, minval=jnp.log(0.3), maxval=jnp.log(3.0)))
    base = jnp.clip(jax.random.normal(jax.random.fold_in(key, 203), (TOKENS, D), jnp.float32), -6.0, 6.0)
    return (0.15 * base * row_scale * col_scale[None, :]).astype(jnp.bfloat16)


def block_scale(key, extent, cuts, low, top_value):
    gain, own = 1.0, jax.random.fold_in(key, 6)
    for dim, parts in cuts:
        heights = jnp.exp(jax.random.uniform(jax.random.fold_in(own, dim), (parts,), jnp.float32, low / len(cuts), top_value / len(cuts)))
        gain = gain * jnp.repeat(heights, extent[dim] // parts).reshape([-1 if axis == dim else 1 for axis in range(len(extent))])
    return gain


def normal_values(stream_key, extent, spread, reach, cuts=(), kind=jnp.bfloat16):
    values = jax.random.normal(stream_key, extent, jnp.float32) * spread
    if len(cuts) > 0:
        values = block_scale(stream_key, extent, cuts, -0.22, 0.18) * values
    return jnp.clip(values, min=-reach, max=reach).astype(kind)


def setup_inputs(seed: int = 0, part: int = 0) -> dict:
    streams_of = jax.random.split(jax.random.key(seed), 11)
    part_keys = jax.random.split(jax.random.fold_in(streams_of[10], part), 11)
    return {
        "tokens": draw_tokens(jax.random.fold_in(jax.random.fold_in(streams_of[10], part), 71), part),
        "group_choice": draw_group_choice(jax.random.fold_in(jax.random.fold_in(streams_of[10], part), 71), part),
        "member_choice": draw_member_choice(jax.random.fold_in(jax.random.fold_in(streams_of[10], part), 71), part),
        "group_prob": jnp.clip(0.3 + 0.7 * jax.random.uniform(part_keys[3], (TOKENS,), jnp.float32) ** block_scale(part_keys[3], (TOKENS,), ((0, 32),), -0.2, 0.2), 0.3, 1.0),
        "member_score": normal_values(part_keys[4], (TOKENS, TOP), 1.5, 4.0, ((0, 32),), jnp.float32),
        "norm_gain": jnp.clip(1.0 + 0.18 * jax.random.normal(streams_of[5], (D,), jnp.float32), 0.1, 1.9),
        "w_gate": normal_values(streams_of[6], (EXPERTS, D, FF), D ** -0.5, 0.09375, ((0, 32), (1, 8))),
        "w_up": normal_values(streams_of[7], (EXPERTS, D, FF), D ** -0.5, 0.09375, ((0, 32), (1, 8))),
        "w_down": normal_values(streams_of[8], (EXPERTS, FF, D), FF ** -0.5, 0.1875, ((0, 32), (2, 8))),
        "final_gain": jnp.clip(1.0 + 0.18 * jax.random.normal(streams_of[9], (D,), jnp.float32), 0.1, 1.9),
    }


EPS = 1e-06

def reference(tokens, group_choice, member_choice, group_prob, member_score, norm_gain, w_gate, w_up, w_down, final_gain):
    values = tokens.astype(jnp.float32)
    square_in = lax.optimization_barrier(jnp.sum(values * values, axis=1, keepdims=True))
    normed = (values * lax.rsqrt(square_in / D + EPS) * norm_gain.astype(jnp.float32)).astype(jnp.bfloat16)
    expert_ids = (group_choice[:, None] * PER_GROUP + member_choice).astype(jnp.int32)
    scores = jnp.exp(member_score)
    weights = group_prob[:, None] * scores / lax.optimization_barrier(jnp.sum(scores, axis=1, keepdims=True))
    blocks = normed.reshape(N_EP, TOK_DEV, D).astype(jnp.float32)
    slot_iota = jnp.arange(CAP, dtype=jnp.int32)

    def one_expert(carried, expert):
        chosen = expert_ids == expert
        counted = lax.optimization_barrier(jnp.sum(chosen.astype(jnp.int32), axis=1)).reshape(N_EP, TOK_DEV)
        weight_mine = lax.optimization_barrier(jnp.sum(jnp.where(chosen, weights, jnp.float32(0.0)), axis=1)).reshape(TOKENS, 1)
        position = jnp.cumsum(counted, axis=1) - counted
        slot_pick = ((position[:, None, :] == slot_iota[None, :, None]) & (counted[:, None, :] > 0)).astype(jnp.float32)
        rows_in = jnp.einsum('sct,std->scd', slot_pick, blocks).astype(jnp.bfloat16)
        rows_in = rows_in.reshape(N_EP * CAP, N_TP, D // N_TP).astype(jnp.float32)
        gate_w = lax.dynamic_index_in_dim(w_gate, expert, 0, keepdims=False).reshape(N_TP, D // N_TP, FF)
        up_w = lax.dynamic_index_in_dim(w_up, expert, 0, keepdims=False).reshape(N_TP, D // N_TP, FF)
        down_w = lax.dynamic_index_in_dim(w_down, expert, 0, keepdims=False)
        gate_part = jnp.einsum('rpd,pdf->prf', rows_in, gate_w.astype(jnp.float32)).astype(jnp.bfloat16)
        up_part = jnp.einsum('rpd,pdf->prf', rows_in, up_w.astype(jnp.float32)).astype(jnp.bfloat16)
        gate_part, up_part = lax.optimization_barrier((gate_part, up_part))
        gate_sum = lax.optimization_barrier(jnp.sum(gate_part.astype(jnp.float32), axis=0))
        up_sum = lax.optimization_barrier(jnp.sum(up_part.astype(jnp.float32), axis=0))
        hidden = (jax.nn.silu(gate_sum) * up_sum).astype(jnp.bfloat16)
        rows_out = jnp.dot(hidden, down_w, preferred_element_type=jnp.float32).astype(jnp.bfloat16)
        rows_out = rows_out.reshape(N_EP, CAP, D).astype(jnp.float32)
        returned = jnp.einsum('sct,scd->std', slot_pick, rows_out).reshape(TOKENS, D)
        return (carried + returned * weight_mine, expert)
    moe, unused = lax.scan(one_expert, jnp.zeros((TOKENS, D), jnp.float32), jnp.arange(EXPERTS, dtype=jnp.int32))
    summed = values + moe
    square_out = lax.optimization_barrier(jnp.sum(summed * summed, axis=1, keepdims=True))
    return (summed * lax.rsqrt(square_out / D + EPS) * final_gain.astype(jnp.float32)).astype(jnp.bfloat16)
```

```python
import functools

import jax
import jax.numpy as jnp
from jax import lax
from jax.experimental import pallas as pl
from jax.experimental.pallas import tpu as pltpu
from jax.sharding import PartitionSpec as P

EPS = 1e-06
F32 = jnp.float32
BF16 = jnp.bfloat16
MESH = pl.DeviceIdType.MESH

CHUNKS = ((1, -1, 2, 0), (-2, 3, -3, 4), (7, -7, 8, -6), (-4, 5, -5, 6))
START = (0, 2, 4, 6)


def dot(a, b):
    return jnp.dot(a, b, preferred_element_type=F32)


def iota(shape, dim):
    return lax.broadcasted_iota(jnp.int32, shape, dim)


def column_of(row, n):
    shape = (n, row.shape[1])
    same = iota(shape, 0) == iota(shape, 1)
    return jnp.sum(jnp.where(same, jnp.broadcast_to(row, shape), 0.0), axis=1, keepdims=True)


def row_of(column, lanes):
    shape = (column.shape[0], lanes)
    same = iota(shape, 0) == iota(shape, 1)
    return jnp.sum(jnp.where(same, jnp.broadcast_to(column, shape), 0.0), axis=0, keepdims=True)


def split3(value):
    first = value.astype(BF16).astype(F32)
    rest = value - first
    second = rest.astype(BF16).astype(F32)
    third = (rest - second).astype(BF16).astype(F32)
    return first, second, third


def kernel(
    dims,
    tokens_ref,
    group_ref,
    member_ref,
    prob_ref,
    score_ref,
    gain_ref,
    final_ref,
    wg_ref,
    wu_ref,
    wd_ref,
    out_ref,
    wgu,
    wdn,
    sorted_buf,
    meta_src,
    rows,
    meta,
    sq_buf,
    sq2_buf,
    rs_send,
    rs_recv,
    hid,
    kept,
    pair_send,
    pair_recv,
    ret_send,
    ret_recv,
    w_sem,
    z_send,
    z_recv,
    m_recv,
    fwd_send,
    fwd_recv,
    mfwd_send,
    mfwd_recv,
    sq_send,
    sq_recv,
    rs_ssem,
    rs_rsem,
    ag_ssem,
    ag_rsem,
    pair_ssem,
    pair_rsem,
    r_recv,
):
    n_z, n_x, groups, width = dims
    per_chips = n_z // groups
    tok, dl = tokens_ref.shape
    cap = tok // groups
    half = n_x // 2
    cols = wgu.shape[2] // 2
    n_rows = rows.shape[1]
    n_mine = n_rows // 2
    ep, me = lax.axis_index("ep"), lax.axis_index("tp")
    z, core = lax.div(ep, 2), lax.rem(ep, 2)
    partner = {"ep": 2 * z + 1 - core}
    right = {"tp": lax.rem(me + 1, n_x)}
    left = {"tp": lax.rem(me + n_x - 1, n_x)}

    def chip(offset):
        return lax.rem(z + offset + n_z, n_z)

    def at_chip(offset):
        return {"ep": 2 * chip(offset) + core}

    def peer(offset):
        return {"tp": lax.rem(me + offset + n_x, n_x)}

    def x_index(offset):
        return lax.rem(me + offset + n_x, n_x)

    def send(src, dst, ssem, rsem, device):
        pltpu.make_async_remote_copy(
            src_ref=src, dst_ref=dst, send_sem=ssem, recv_sem=rsem, device_id=device, device_id_type=MESH
        ).start()

    def await_bytes(ref, sem):
        pltpu.make_async_copy(ref, ref, sem).wait()

    barrier = pltpu.get_barrier_semaphore()
    greeted = [at_chip(k) for k in range(1, n_z)] + [partner] + [peer(k) for k in range(1, n_x)]
    for device in greeted:
        pl.semaphore_signal(barrier, inc=1, device_id=device, device_id_type=MESH)

    loads = []
    for o in range(n_x):
        span = pl.ds(o * cols, cols)
        loads.append(pltpu.make_async_copy(wg_ref.at[0, :, span], wgu.at[o, :, pl.ds(0, cols)], w_sem.at[0]))
        loads.append(pltpu.make_async_copy(wu_ref.at[0, :, span], wgu.at[o, :, pl.ds(cols, cols)], w_sem.at[0]))
    loads.append(pltpu.make_async_copy(wd_ref.at[0], wdn, w_sem.at[1]))
    for load in loads:
        load.start()

    values = tokens_ref[...].astype(F32)
    scaled = (values * gain_ref[...]).astype(BF16)
    group_row = group_ref[...]
    chosen = (iota((8, tok), 0) == jnp.broadcast_to(group_row, (8, tok))).astype(F32)
    earlier = (iota((tok, tok), 0) < iota((tok, tok), 1)).astype(F32)
    rank = jnp.sum(dot(chosen, earlier) * chosen, axis=0, keepdims=True)
    slot_row = group_row.astype(F32) * cap + rank
    slot_col = column_of(slot_row, tok)
    picker = (iota((tok, tok), 0).astype(F32) == jnp.broadcast_to(slot_row, (tok, tok))).astype(BF16)
    sorted_buf[...] = dot(picker, scaled).astype(BF16)
    square = jnp.sum(values * values, axis=1, keepdims=True)
    sq_buf[pl.ds(me, 1)] = row_of(square, 128).reshape(1, 1, 128)

    def block_of(offset):
        g = lax.div(chip(-offset), per_chips)
        return pl.ds(pl.multiple_of(g * cap, cap), cap)

    pl.semaphore_wait(barrier, len(greeted))

    for c, offsets in enumerate(CHUNKS):
        for j, offset in enumerate(offsets):
            place = pl.ds(j * cap, cap)
            if offset == 0:
                rows[c, place, :] = sorted_buf[block_of(0), :]
            else:
                send(sorted_buf.at[block_of(offset)], rows.at[c, place], z_send.at[0], z_recv.at[c], at_chip(-offset))
    for k in range(1, n_x):
        send(sq_buf.at[me], sq_buf.at[me], sq_send.at[0], sq_recv.at[0], peer(k))

    def remote_rows(c):
        return pl.ds(0, cap * sum(1 for offset in CHUNKS[c] if offset != 0))

    def take(c):
        await_bytes(rows.at[c, remote_rows(c)], z_recv.at[c])
        send(rows.at[c, pl.ds(0, n_mine)], rows.at[c, pl.ds(n_mine, n_mine)], fwd_send.at[c], fwd_recv.at[c], partner)

    def send_meta():
        await_bytes(sq_buf.at[pl.ds(0, n_x - 1)], sq_recv.at[0])
        total = column_of(jnp.sum(sq_buf[...], axis=0), tok)
        factor = lax.rsqrt(total / width + EPS)
        score = jnp.exp(score_ref[...])
        weight = column_of(prob_ref[...], tok) * score / jnp.sum(score, axis=1, keepdims=True)
        lane = iota((tok, 128), 1)
        dense = jnp.zeros((tok, 128), F32)
        for k in range(member_ref.shape[1]):
            named = lax.rem(lane, 8) == member_ref[:, k : k + 1]
            dense = jnp.where(named, weight[:, k : k + 1], dense)
        parts = split3(dense)
        factors = split3(factor)
        packed = jnp.zeros((tok, 128), F32)
        for k in range(3):
            packed = jnp.where(lax.div(lane, 8) == k, parts[k], packed)
            packed = jnp.where(lane == 24 + k, factors[k], packed)
        meta_src[...] = dot(picker, packed.astype(BF16)).astype(BF16)
        for c, offsets in enumerate(CHUNKS):
            for j, offset in enumerate(offsets):
                place = pl.ds(j * cap, cap)
                if offset == 0:
                    meta[c, place, :] = meta_src[block_of(0), :]
                else:
                    send(meta_src.at[block_of(offset)], meta.at[c, place], z_send.at[1], m_recv.at[c], at_chip(-offset))

    def pass_meta(c):
        await_bytes(meta.at[c, remote_rows(c)], m_recv.at[c])
        send(meta.at[c, pl.ds(0, n_mine)], meta.at[c, pl.ds(n_mine, n_mine)], mfwd_send.at[c], mfwd_recv.at[c], partner)

    gate_cols, up_cols = pl.ds(0, cols), pl.ds(cols, cols)

    def partial(c, owner):
        return dot(rows[c], wgu[owner])

    def reduce_step(c, s):
        if s == 0:
            both = partial(c, x_index(half)).astype(BF16)
            rs_send[c, 0, 0, :, cols:] = both[:, cols:]
            rs_send[c, 0, 1, :, :cols] = both[:, :cols]
            send(rs_send.at[c, 0, 0, :, up_cols], rs_recv.at[c, 0, 0, :, up_cols], rs_ssem.at[c, 0, 0], rs_rsem.at[c, 0, 0], right)
            send(rs_send.at[c, 0, 1, :, gate_cols], rs_recv.at[c, 0, 1, :, gate_cols], rs_ssem.at[c, 0, 1], rs_rsem.at[c, 0, 1], left)
            return
        for d, (sign, device) in enumerate(((1, right), (-1, left))):
            mine = partial(c, x_index(sign * (half - s)))
            await_reduce(c, s - 1, d)
            if s == 1:
                lo, hi = (0, cols) if d == 0 else (cols, 2 * cols)
                alone = slice(lo, hi)
                other = slice(cols - lo, 2 * cols - lo)
                rs_send[c, s, d, :, alone] = mine[:, alone].astype(BF16)
                rs_send[c, s, d, :, other] = (mine[:, other] + rs_recv[c, s - 1, d, :, other].astype(F32)).astype(BF16)
            else:
                rs_send[c, s, d] = (mine + rs_recv[c, s - 1, d].astype(F32)).astype(BF16)
            send(rs_send.at[c, s, d], rs_recv.at[c, s, d], rs_ssem.at[c, s, d], rs_rsem.at[c, s, d], device)

    def reduce_ref(buf, c, s, d):
        if s > 0:
            return buf.at[c, s, d]
        return buf.at[c, s, d, :, up_cols if d == 0 else gate_cols]

    def await_reduce(c, s, d):
        await_bytes(reduce_ref(rs_recv, c, s, d), rs_rsem.at[c, s, d])

    def gather_ref(c, s, d, owner):
        if s < half - 1:
            return hid.at[c, owner]
        return hid.at[c, owner, pl.ds(d * n_mine, n_mine)]

    def gather_send(c, s):
        for d, (sign, device) in enumerate(((1, right), (-1, left))):
            block = gather_ref(c, s, d, x_index(-sign * s))
            send(block, block, ag_ssem.at[c, s, d], ag_rsem.at[c, s, d], device)

    def gather_wait(c, s):
        for d, sign in enumerate((1, -1)):
            await_bytes(gather_ref(c, s, d, x_index(-sign * (s + 1))), ag_rsem.at[c, s, d])

    def activate(c):
        total = partial(c, me)
        await_bytes(meta.at[c, pl.ds(n_mine, n_mine)], mfwd_recv.at[c])
        lane = iota((n_rows, 128), 1)
        info = meta[c].astype(F32)
        factor = jnp.sum(jnp.where(lax.div(lane, 8) == 3, info, 0.0), axis=1, keepdims=True)
        for d in range(2):
            await_reduce(c, half - 1, d)
            total = total + rs_recv[c, half - 1, d].astype(F32)
        total = total * factor
        gate, up = total[:, :cols], total[:, cols:]
        hid[c, me] = (gate / (1.0 + jnp.exp(-gate)) * up).astype(BF16)
        gather_send(c, 0)

    def produce(c):
        gather_wait(c, half - 1)
        hidden = jnp.concatenate([hid[c, o] for o in range(n_x)], axis=1)
        made = dot(hidden, wdn[...])
        lane = iota((n_rows, 128), 1)
        info = meta[c].astype(F32)
        member = 2 * lax.rem(z, per_chips) + core
        named = (lax.rem(lane, 8) == member) & (lane < 24)
        weight = jnp.sum(jnp.where(named, info, 0.0), axis=1, keepdims=True)
        made = made.astype(BF16).astype(F32) * weight
        pair_send[c] = made[n_mine:].astype(BF16)
        send(pair_send.at[c], pair_recv.at[c], pair_ssem.at[c], pair_rsem.at[c], partner)
        kept[c] = made[:n_mine]

    def give_back(c):
        await_bytes(pair_recv.at[c], pair_rsem.at[c])
        ret_send[c] = (kept[c] + pair_recv[c].astype(F32)).astype(BF16)
        for j, offset in enumerate(CHUNKS[c]):
            place = pl.ds(j * cap, cap)
            if offset == 0:
                ret_recv[c, place, :] = ret_send[c, place, :]
            else:
                send(ret_send.at[c, place], ret_recv.at[c, place], z_send.at[2], r_recv.at[c], at_chip(offset))

    def stage(c, k):
        if k == 0:
            await_bytes(rows.at[c, pl.ds(n_mine, n_mine)], fwd_recv.at[c])
            reduce_step(c, 0)
        elif k < half:
            reduce_step(c, k)
            if k == half - 2:
                pass_meta(c)
        elif k == half:
            activate(c)
        elif k < 2 * half:
            gather_wait(c, k - half - 1)
            gather_send(c, k - half)
        elif k == 2 * half:
            produce(c)
        else:
            give_back(c)

    last = 2 * half + 1
    n_chunks = len(CHUNKS)
    for t in range(max(START) + last + 1):
        for c in range(n_chunks):
            if t == max(START[c] - 1, 0) and (c == 0 or t > 0):
                take(c)
        if t == 0:
            await_bytes(wgu, w_sem.at[0])
        for c in range(n_chunks):
            k = t - START[c]
            if 0 <= k <= last:
                stage(c, k)
        if t == 0:
            send_meta()
            await_bytes(wdn, w_sem.at[1])

    moe = jnp.zeros((tok, dl), F32)
    for c, offsets in enumerate(CHUNKS):
        await_bytes(ret_recv.at[c, remote_rows(c)], r_recv.at[c])
        lane = iota((1, n_mine), 1)
        slots = lax.rem(lane, cap)
        for j, offset in enumerate(offsets):
            slots = slots + jnp.where(lax.div(lane, cap) == j, lax.div(chip(-offset), per_chips) * cap, 0)
        unpick = (jnp.broadcast_to(slot_col, (tok, n_mine)) == jnp.broadcast_to(slots.astype(F32), (tok, n_mine))).astype(BF16)
        moe = moe + dot(unpick, ret_recv[c])
    summed = tokens_ref[...].astype(F32) + moe
    square = jnp.sum(summed * summed, axis=1, keepdims=True)
    sq2_buf[pl.ds(me, 1)] = row_of(square, 128).reshape(1, 1, 128)
    for k in range(1, n_x):
        send(sq2_buf.at[me], sq2_buf.at[me], sq_send.at[1], sq_recv.at[1], peer(k))
    await_bytes(sq2_buf.at[pl.ds(0, n_x - 1)], sq_recv.at[1])
    total = column_of(jnp.sum(sq2_buf[...], axis=0), tok)
    out_ref[...] = (summed * lax.rsqrt(total / width + EPS) * final_ref[...]).astype(BF16)

    n_remote = cap * (n_z - 1)
    flat = wdn.at[pl.ds(0, n_remote)]
    await_bytes(flat, z_send.at[0])
    await_bytes(wdn.at[pl.ds(0, n_remote), pl.ds(0, 128)], z_send.at[1])
    await_bytes(flat, z_send.at[2])
    await_bytes(sq_buf.at[pl.ds(0, n_x - 1)], sq_send.at[0])
    await_bytes(sq_buf.at[pl.ds(0, n_x - 1)], sq_send.at[1])
    for c in range(n_chunks):
        await_bytes(rows.at[c, pl.ds(0, n_mine)], fwd_send.at[c])
        await_bytes(meta.at[c, pl.ds(0, n_mine)], mfwd_send.at[c])
        await_bytes(pair_recv.at[c], pair_ssem.at[c])
        for s in range(half):
            for d in range(2):
                await_bytes(reduce_ref(rs_send, c, s, d), rs_ssem.at[c, s, d])
                await_bytes(gather_ref(c, s, d, me), ag_ssem.at[c, s, d])


def local(tokens, group_choice, member_choice, group_prob, member_score, norm_gain, w_gate, w_up, w_down, final_gain):
    n_z, n_x = lax.axis_size("ep") // 2, lax.axis_size("tp")
    groups = max(2, 2 * n_z // 8)
    tok, dl = tokens.shape
    ff = w_gate.shape[2]
    cap = tok // groups
    cols = ff // n_x
    n_chunks = len(CHUNKS)
    n_mine = cap * len(CHUNKS[0])
    n_rows = 2 * n_mine
    half = n_x // 2
    dma = pltpu.SemaphoreType.DMA
    vmem = pl.BlockSpec(memory_space=pltpu.VMEM)
    hbm = pl.BlockSpec(memory_space=pl.ANY)
    return pl.pallas_call(
        functools.partial(kernel, (n_z, n_x, groups, dl * n_x)),
        out_shape=jax.ShapeDtypeStruct((tok, dl), BF16),
        in_specs=[vmem] * 7 + [hbm] * 3,
        out_specs=vmem,
        scratch_shapes=[
            pltpu.VMEM((n_x, dl, 2 * cols), BF16),
            pltpu.VMEM((ff, dl), BF16),
            pltpu.VMEM((tok, dl), BF16),
            pltpu.VMEM((tok, 128), BF16),
            pltpu.VMEM((n_chunks, n_rows, dl), BF16),
            pltpu.VMEM((n_chunks, n_rows, 128), BF16),
            pltpu.VMEM((n_x, 1, 128), F32),
            pltpu.VMEM((n_x, 1, 128), F32),
            pltpu.VMEM((n_chunks, half, 2, n_rows, 2 * cols), BF16),
            pltpu.VMEM((n_chunks, half, 2, n_rows, 2 * cols), BF16),
            pltpu.VMEM((n_chunks, n_x, n_rows, cols), BF16),
            pltpu.VMEM((n_chunks, n_mine, dl), F32),
            pltpu.VMEM((n_chunks, n_mine, dl), BF16),
            pltpu.VMEM((n_chunks, n_mine, dl), BF16),
            pltpu.VMEM((n_chunks, n_mine, dl), BF16),
            pltpu.VMEM((n_chunks, n_mine, dl), BF16),
            dma((2,)),
            dma((3,)),
            dma((n_chunks,)),
            dma((n_chunks,)),
            dma((n_chunks,)),
            dma((n_chunks,)),
            dma((n_chunks,)),
            dma((n_chunks,)),
            dma((2,)),
            dma((2,)),
            dma((n_chunks, half, 2)),
            dma((n_chunks, half, 2)),
            dma((n_chunks, half, 2)),
            dma((n_chunks, half, 2)),
            dma((n_chunks,)),
            dma((n_chunks,)),
            dma((n_chunks,)),
        ],
        compiler_params=pltpu.CompilerParams(
            collective_id=0, has_side_effects=True, vmem_limit_bytes=48 * 1024 * 1024
        ),
    )(
        tokens,
        group_choice.reshape(1, tok),
        member_choice,
        group_prob.reshape(1, tok),
        member_score,
        norm_gain.reshape(1, dl),
        final_gain.reshape(1, dl),
        w_gate,
        w_up,
        w_down,
    )


def solution(mesh):
    rows = ("grp", "ep")
    placed = (
        P(rows, "tp"),
        P(rows),
        P(rows, None),
        P(rows),
        P(rows, None),
        P("tp"),
        P("ep", "tp", None),
        P("ep", "tp", None),
        P("ep", None, "tp"),
        P("tp"),
    )
    return jax.shard_map(local, mesh=mesh, in_specs=placed, out_specs=P(rows, "tp"), check_vma=False)
```

```python
import functools

import jax
import jax.numpy as jnp
from jax import lax
from jax.experimental import pallas as pl
from jax.experimental.pallas import tpu as pltpu
from jax.sharding import PartitionSpec as P

EPS = 1e-06
F32 = jnp.float32
BF16 = jnp.bfloat16
MESH = pl.DeviceIdType.MESH

CHUNKS = (4, 4, 4, 4)
START = (0, 1, 2, 3)


def dot(a, b):
    return jnp.dot(a, b, preferred_element_type=F32)


def iota(shape, dim):
    return lax.broadcasted_iota(jnp.int32, shape, dim)


def column_of(row, n):
    shape = (n, row.shape[1])
    same = iota(shape, 0) == iota(shape, 1)
    return jnp.sum(jnp.where(same, jnp.broadcast_to(row, shape), 0.0), axis=1, keepdims=True)


def row_of(column, lanes):
    shape = (column.shape[0], lanes)
    same = iota(shape, 0) == iota(shape, 1)
    return jnp.sum(jnp.where(same, jnp.broadcast_to(column, shape), 0.0), axis=0, keepdims=True)


def split3(value):
    first = value.astype(BF16).astype(F32)
    rest = value - first
    second = rest.astype(BF16).astype(F32)
    third = (rest - second).astype(BF16).astype(F32)
    return first, second, third


def kernel(
    dims,
    tokens_ref,
    group_ref,
    member_ref,
    prob_ref,
    score_ref,
    gain_ref,
    final_ref,
    wg_ref,
    wu_ref,
    wd_ref,
    out_ref,
    wgu,
    wdn,
    sorted_buf,
    meta_src,
    rows_mine,
    rows_other,
    meta_mine,
    meta_other,
    sq_buf,
    sq2_buf,
    rs_send,
    rs_recv,
    hid,
    kept,
    pair_send,
    pair_recv,
    ret_send,
    ret_recv,
    summed_buf,
    w_sem,
    z_send,
    z_recv,
    m_recv,
    r_recv,
    fwd_send,
    fwd_recv,
    mfwd_send,
    mfwd_recv,
    sq_send,
    sq_recv,
    rs_ssem,
    rs_rsem,
    ag_ssem,
    ag_rsem,
    pair_ssem,
    pair_rsem,
    here_z,
    here_x,
    here_c,
):
    n_z, n_x, groups, width = dims
    per_chips = n_z // groups
    tok, dl = tokens_ref.shape
    cap = tok // groups
    half = n_x // 2
    cols = wgu.shape[2] // 2
    n_chunks = len(CHUNKS)
    bases = [sum(CHUNKS[:c]) for c in range(n_chunks)]
    ep, me = lax.axis_index("ep"), lax.axis_index("tp")
    z, core = lax.div(ep, 2), lax.rem(ep, 2)
    partner = {"ep": 2 * z + 1 - core}
    right = {"tp": lax.rem(me + 1, n_x)}
    left = {"tp": lax.rem(me + n_x - 1, n_x)}

    def at_chip(k):
        return {"ep": 2 * k + core}

    def x_index(offset):
        return lax.rem(me + offset + n_x, n_x)

    def block(index):
        return pl.ds(pl.multiple_of(index * cap, cap), cap)

    def span(c):
        return pl.ds(bases[c] * cap, CHUNKS[c] * cap)

    def n_mine(c):
        return CHUNKS[c] * cap

    def in_chunk(c):
        return (z >= bases[c]) & (z < bases[c] + CHUNKS[c])

    def send(src, dst, ssem, rsem, device):
        pltpu.make_async_remote_copy(
            src_ref=src, dst_ref=dst, send_sem=ssem, recv_sem=rsem, device_id=device, device_id_type=MESH
        ).start()

    def await_bytes(ref, sem):
        pltpu.make_async_copy(ref, ref, sem).wait()

    def signal(sem, device):
        pl.semaphore_signal(sem, inc=1, device_id=device, device_id_type=MESH)

    def each(lo, hi, body):
        def step(i, carry):
            body(i)
            return carry

        lax.fori_loop(lo, hi, step, 0)

    def ranked(index, n, odd):
        moved = jnp.where(index == 0, n - 2, jnp.where(index == n - 1, n - 1, index - 1))
        return jnp.where(odd, moved, index)

    def unranked(rank, n, odd):
        moved = jnp.where(rank == n - 2, 0, jnp.where(rank == n - 1, n - 1, rank + 1))
        return jnp.where(odd, moved, rank)

    def folded(index):
        return jnp.where(index < half, index, n_x - 1 - index + half)

    z_odd, x_odd, c_odd = (me == 0) & (core == 0), (z == 0) & (core == 0), (z == 0) & (me == 0)
    z_rank = ranked(z, n_z, z_odd)
    x_rank = jnp.where(x_odd, lax.rem(folded(me) + n_x - 1, n_x), folded(me))
    c_rank = jnp.where(c_odd, 1 - core, core)

    def z_of(rank):
        return unranked(rank, n_z, z_odd)

    def x_of(rank):
        return folded(jnp.where(x_odd, lax.rem(rank + 1, n_x), rank))

    barrier = pltpu.get_barrier_semaphore()
    each(z_rank + 1, n_z, lambda r: signal(barrier, at_chip(z_of(r))))
    each(x_rank + 1, n_x, lambda r: signal(barrier, {"tp": x_of(r)}))

    @pl.when(c_rank == 0)
    def _():
        signal(barrier, partner)

    loads = []
    for o in range(n_x):
        part = pl.ds(o * cols, cols)
        loads.append(pltpu.make_async_copy(wg_ref.at[0, :, part], wgu.at[o, :, pl.ds(0, cols)], w_sem.at[0]))
        loads.append(pltpu.make_async_copy(wu_ref.at[0, :, part], wgu.at[o, :, pl.ds(cols, cols)], w_sem.at[0]))
    loads.append(pltpu.make_async_copy(wd_ref.at[0], wdn, w_sem.at[1]))
    for load in loads:
        load.start()

    values = tokens_ref[...].astype(F32)
    scaled = (values * gain_ref[...]).astype(BF16)
    group_row = group_ref[...]
    chosen = (iota((8, tok), 0) == jnp.broadcast_to(group_row, (8, tok))).astype(F32)
    earlier = (iota((tok, tok), 0) < iota((tok, tok), 1)).astype(F32)
    rank = jnp.sum(dot(chosen, earlier) * chosen, axis=0, keepdims=True)
    slot_row = group_row.astype(F32) * cap + rank
    picker = (iota((tok, tok), 0).astype(F32) == jnp.broadcast_to(slot_row, (tok, tok))).astype(BF16)
    sorted_buf[...] = dot(picker, scaled).astype(BF16)
    square = jnp.sum(values * values, axis=1, keepdims=True)
    sq_buf[pl.ds(me, 1)] = row_of(square, 128).reshape(1, 1, 128)
    rows_mine[block(z), :] = sorted_buf[block(lax.div(z, per_chips)), :]

    def send_rows(k):
        send(sorted_buf.at[block(lax.div(k, per_chips))], rows_mine.at[block(z)], z_send.at[0], z_recv.at[z], at_chip(k))

    def send_meta(k):
        send(meta_src.at[block(lax.div(k, per_chips))], meta_mine.at[block(z)], z_send.at[1], m_recv.at[z], at_chip(k))

    with jax.named_scope("meet"):
        expected = z_rank + x_rank + c_rank

        @pl.when(expected > 0)
        def _():
            pl.semaphore_wait(barrier, expected)

        each(0, z_rank, lambda r: signal(here_z.at[z], at_chip(z_of(r))))
        each(0, x_rank, lambda r: signal(here_x.at[me], {"tp": x_of(r)}))

        @pl.when(c_rank == 1)
        def _():
            signal(here_c, partner)

    def greet(r):
        k = z_of(r)
        pl.semaphore_wait(here_z.at[k], 1)
        send_rows(k)

    with jax.named_scope("greet"):
        each(0, z_rank, lambda r: send_rows(z_of(r)))
        each(z_rank + 1, n_z, greet)

    def send_square(r):
        send(sq_buf.at[me], sq_buf.at[me], sq_send.at[0], sq_recv.at[0], {"tp": x_of(r)})

    def greet_x(r):
        pl.semaphore_wait(here_x.at[x_of(r)], 1)
        send_square(r)

    with jax.named_scope("greet_x"):
        each(0, x_rank, send_square)
        each(x_rank + 1, n_x, greet_x)

        @pl.when(c_rank == 0)
        def _():
            pl.semaphore_wait(here_c, 1)

    def await_blocks(c, ref, sems):
        for k in range(bases[c], bases[c] + CHUNKS[c]):

            @pl.when(z != k)
            def _(k=k):
                await_bytes(ref.at[pl.ds(k * cap, cap)], sems.at[k])

    def take(c):
        await_blocks(c, rows_mine, z_recv)
        send(rows_mine.at[span(c)], rows_other.at[span(c)], fwd_send.at[c], fwd_recv.at[c], partner)

    def make_meta():
        await_bytes(sq_buf.at[pl.ds(0, n_x - 1)], sq_recv.at[0])
        total = jnp.sum(sq_buf[...], axis=0)[:, :tok]
        factor = lax.rsqrt(total / width + EPS)
        score = jnp.exp(score_ref[...])
        weight = prob_ref[...] * score / jnp.sum(score, axis=0, keepdims=True)
        member = iota((8, tok), 0)
        dense = jnp.zeros((8, tok), F32)
        for k in range(member_ref.shape[0]):
            dense = jnp.where(member == member_ref[k : k + 1, :], weight[k : k + 1, :], dense)
        parts = split3(dense)
        factors = split3(factor)
        spread = jnp.zeros((8, tok), F32)
        for k in range(3):
            spread = jnp.where(member == k, factors[k], spread)
        packed = jnp.concatenate([*parts, spread, jnp.zeros((96, tok), F32)], axis=0)
        meta_src[...] = lax.dot_general(
            picker, packed.astype(BF16), (((1,), (1,)), ((), ())), preferred_element_type=F32
        ).astype(BF16)
        meta_mine[block(z), :] = meta_src[block(lax.div(z, per_chips)), :]
        each(0, z_rank, lambda r: send_meta(z_of(r)))
        each(z_rank + 1, n_z, lambda r: send_meta(z_of(r)))

    def pass_meta(c):
        await_blocks(c, meta_mine, m_recv)
        send(meta_mine.at[span(c)], meta_other.at[span(c)], mfwd_send.at[c], mfwd_recv.at[c], partner)

    gate_cols, up_cols = pl.ds(0, cols), pl.ds(cols, cols)

    def partial(c, owner):
        both = jnp.concatenate([rows_mine[span(c), :], rows_other[span(c), :]], axis=0)
        return dot(both, wgu[owner])

    def reduce_ref(buf, c, s, d):
        used = pl.ds(0, 2 * n_mine(c))
        if s > 0:
            return buf.at[c, s, d, used]
        return buf.at[c, s, d, used, up_cols if d == 0 else gate_cols]

    def await_reduce(c, s, d):
        await_bytes(reduce_ref(rs_recv, c, s, d), rs_rsem.at[c, s, d])

    def reduce_send(c, s, d):
        send(
            reduce_ref(rs_send, c, s, d),
            reduce_ref(rs_recv, c, s, d),
            rs_ssem.at[c, s, d],
            rs_rsem.at[c, s, d],
            right if d == 0 else left,
        )

    def reduce_step(c, s):
        n = 2 * n_mine(c)
        if s == 0:
            both = partial(c, x_index(half)).astype(BF16)
            rs_send[c, 0, 0, :n, cols:] = both[:, cols:]
            rs_send[c, 0, 1, :n, :cols] = both[:, :cols]
            reduce_send(c, 0, 0)
            reduce_send(c, 0, 1)
            return
        for d, sign in enumerate((1, -1)):
            mine = partial(c, x_index(sign * (half - s)))
            await_reduce(c, s - 1, d)
            if s == 1:
                lo = d * cols
                alone = slice(lo, lo + cols)
                other = slice(cols - lo, 2 * cols - lo)
                rs_send[c, s, d, :n, alone] = mine[:, alone].astype(BF16)
                rs_send[c, s, d, :n, other] = (mine[:, other] + rs_recv[c, s - 1, d, :n, other].astype(F32)).astype(BF16)
            else:
                rs_send[c, s, d, :n] = (mine + rs_recv[c, s - 1, d, :n].astype(F32)).astype(BF16)
            reduce_send(c, s, d)

    def gather_ref(c, s, d, owner):
        if s < half - 1:
            return hid.at[c, owner, pl.ds(0, 2 * n_mine(c))]
        return hid.at[c, owner, pl.ds(d * n_mine(c), n_mine(c))]

    def gather_send(c, s):
        for d, sign in enumerate((1, -1)):
            ref = gather_ref(c, s, d, x_index(-sign * s))
            send(ref, ref, ag_ssem.at[c, s, d], ag_rsem.at[c, s, d], right if d == 0 else left)

    def gather_wait(c, s):
        for d, sign in enumerate((1, -1)):
            await_bytes(gather_ref(c, s, d, x_index(-sign * (s + 1))), ag_rsem.at[c, s, d])

    def info(c):
        return jnp.concatenate([meta_mine[span(c), :], meta_other[span(c), :]], axis=0).astype(F32)

    def activate(c):
        n = 2 * n_mine(c)
        total = partial(c, me)
        await_bytes(meta_other.at[span(c)], mfwd_recv.at[c])
        lane = iota((n, 128), 1)
        factor = jnp.sum(jnp.where(lax.div(lane, 8) == 3, info(c), 0.0), axis=1, keepdims=True)
        for d in range(2):
            await_reduce(c, half - 1, d)
            total = total + rs_recv[c, half - 1, d, :n].astype(F32)
        total = total * factor
        gate, up = total[:, :cols], total[:, cols:]
        hid[c, me, :n] = (gate / (1.0 + jnp.exp(-gate)) * up).astype(BF16)
        gather_send(c, 0)

    def produce(c):
        n = 2 * n_mine(c)
        gather_wait(c, half - 1)
        hidden = jnp.concatenate([hid[c, o, :n] for o in range(n_x)], axis=1)
        made = dot(hidden, wdn[...])
        lane = iota((n, 128), 1)
        member = 2 * lax.rem(z, per_chips) + core
        named = (lax.rem(lane, 8) == member) & (lane < 24)
        weight = jnp.sum(jnp.where(named, info(c), 0.0), axis=1, keepdims=True)
        made = made.astype(BF16).astype(F32) * weight
        pair_send[span(c), :] = made[n_mine(c) :].astype(BF16)
        send(pair_send.at[span(c)], pair_recv.at[span(c)], pair_ssem.at[c], pair_rsem.at[c], partner)
        kept[span(c), :] = made[: n_mine(c)]

    def give_back(c):
        await_bytes(pair_recv.at[span(c)], pair_rsem.at[c])
        ret_send[span(c), :] = (kept[span(c), :] + pair_recv[span(c), :].astype(F32)).astype(BF16)
        for k in range(bases[c], bases[c] + CHUNKS[c]):

            @pl.when(z == k)
            def _(k=k):
                ret_recv[block(k), :] = ret_send[block(k), :]

            @pl.when(z != k)
            def _(k=k):
                send(ret_send.at[block(k)], ret_recv.at[block(z)], z_send.at[2], r_recv.at[z], at_chip(k))

    def gather_returned():
        for k in range(n_z):

            @pl.when(z != k)
            def _(k=k):
                await_bytes(ret_recv.at[block(k)], r_recv.at[k])

        row = iota((n_z * cap, tok), 0)
        slots = lax.div(row, per_chips * cap) * cap + lax.rem(row, cap)
        unpick = (slots.astype(F32) == jnp.broadcast_to(slot_row, row.shape)).astype(BF16)
        moe = lax.dot_general(unpick, ret_recv[...], (((0,), (0,)), ((), ())), preferred_element_type=F32)
        summed = tokens_ref[...].astype(F32) + moe
        summed_buf[...] = summed
        total = jnp.sum(summed * summed, axis=1, keepdims=True)
        sq2_buf[pl.ds(me, 1)] = row_of(total, 128).reshape(1, 1, 128)

        def send_total(r):
            send(sq2_buf.at[me], sq2_buf.at[me], sq_send.at[1], sq_recv.at[1], {"tp": r})

        each(0, me, send_total)
        each(me + 1, n_x, send_total)

    def write_out():
        await_bytes(sq2_buf.at[pl.ds(0, n_x - 1)], sq_recv.at[1])
        total = column_of(jnp.sum(sq2_buf[...], axis=0), tok)
        out_ref[...] = (summed_buf[...] * lax.rsqrt(total / width + EPS) * final_ref[...]).astype(BF16)

    def stage(c, k):
        if k == 0:
            await_bytes(rows_other.at[span(c)], fwd_recv.at[c])
            reduce_step(c, 0)
        elif k < half:
            reduce_step(c, k)
            if k == half - 2:
                pass_meta(c)
        elif k == half:
            activate(c)
        elif k < 2 * half:
            gather_wait(c, k - half - 1)
            gather_send(c, k - half)
        elif k == 2 * half:
            produce(c)
        else:
            give_back(c)

    last = 2 * half + 1
    with jax.named_scope("take#c=0"):
        take(0)
    with jax.named_scope("weights"):
        await_bytes(wgu, w_sem.at[0])
        await_bytes(wdn, w_sem.at[1])
    for t in range(START[-1] + last + 1):
        for c in range(n_chunks):
            k = t - START[c]
            if 0 <= k <= last:
                with jax.named_scope(f"stage#c={c}#k={k}"):
                    stage(c, k)
            if k == -1:
                with jax.named_scope(f"take#c={c}"):
                    take(c)
        if t == 1:
            with jax.named_scope("make_meta"):
                make_meta()
    with jax.named_scope("returned"):
        gather_returned()
    with jax.named_scope("write"):
        write_out()

    n_remote = cap * (n_z - 1)
    flat = wdn.at[pl.ds(0, n_remote)]
    await_bytes(flat, z_send.at[0])
    await_bytes(wdn.at[pl.ds(0, n_remote), pl.ds(0, 128)], z_send.at[1])
    await_bytes(flat, z_send.at[2])
    await_bytes(sq_buf.at[pl.ds(0, n_x - 1)], sq_send.at[0])
    await_bytes(sq_buf.at[pl.ds(0, n_x - 1)], sq_send.at[1])
    for c in range(n_chunks):
        await_bytes(rows_mine.at[span(c)], fwd_send.at[c])
        await_bytes(meta_mine.at[span(c)], mfwd_send.at[c])
        await_bytes(pair_recv.at[span(c)], pair_ssem.at[c])
        for s in range(half):
            for d in range(2):
                await_bytes(reduce_ref(rs_send, c, s, d), rs_ssem.at[c, s, d])
                await_bytes(gather_ref(c, s, d, me), ag_ssem.at[c, s, d])


def local(tokens, group_choice, member_choice, group_prob, member_score, norm_gain, w_gate, w_up, w_down, final_gain):
    n_z, n_x = lax.axis_size("ep") // 2, lax.axis_size("tp")
    groups = max(2, 2 * n_z // 8)
    tok, dl = tokens.shape
    ff = w_gate.shape[2]
    cap = tok // groups
    cols = ff // n_x
    n_chunks = len(CHUNKS)
    n_rows = 2 * cap * max(CHUNKS)
    n_all = n_z * cap
    half = n_x // 2
    dma = pltpu.SemaphoreType.DMA
    vmem = pl.BlockSpec(memory_space=pltpu.VMEM)
    hbm = pl.BlockSpec(memory_space=pl.ANY)
    return pl.pallas_call(
        functools.partial(kernel, (n_z, n_x, groups, dl * n_x)),
        out_shape=jax.ShapeDtypeStruct((tok, dl), BF16),
        in_specs=[vmem] * 7 + [hbm] * 3,
        out_specs=vmem,
        scratch_shapes=[
            pltpu.VMEM((n_x, dl, 2 * cols), BF16),
            pltpu.VMEM((ff, dl), BF16),
            pltpu.VMEM((tok, dl), BF16),
            pltpu.VMEM((tok, 128), BF16),
            pltpu.VMEM((n_all, dl), BF16),
            pltpu.VMEM((n_all, dl), BF16),
            pltpu.VMEM((n_all, 128), BF16),
            pltpu.VMEM((n_all, 128), BF16),
            pltpu.VMEM((n_x, 1, 128), F32),
            pltpu.VMEM((n_x, 1, 128), F32),
            pltpu.VMEM((n_chunks, half, 2, n_rows, 2 * cols), BF16),
            pltpu.VMEM((n_chunks, half, 2, n_rows, 2 * cols), BF16),
            pltpu.VMEM((n_chunks, n_x, n_rows, cols), BF16),
            pltpu.VMEM((n_all, dl), F32),
            pltpu.VMEM((n_all, dl), BF16),
            pltpu.VMEM((n_all, dl), BF16),
            pltpu.VMEM((n_all, dl), BF16),
            pltpu.VMEM((n_all, dl), BF16),
            pltpu.VMEM((tok, dl), F32),
            dma((2,)),
            dma((3,)),
            dma((n_z,)),
            dma((n_z,)),
            dma((n_z,)),
            dma((n_chunks,)),
            dma((n_chunks,)),
            dma((n_chunks,)),
            dma((n_chunks,)),
            dma((2,)),
            dma((2,)),
            dma((n_chunks, half, 2)),
            dma((n_chunks, half, 2)),
            dma((n_chunks, half, 2)),
            dma((n_chunks, half, 2)),
            dma((n_chunks,)),
            dma((n_chunks,)),
            pltpu.SemaphoreType.REGULAR((n_z,)),
            pltpu.SemaphoreType.REGULAR((n_x,)),
            pltpu.SemaphoreType.REGULAR,
        ],
        compiler_params=pltpu.CompilerParams(
            collective_id=0, has_side_effects=True, vmem_limit_bytes=67043328
        ),
    )(
        tokens,
        group_choice.reshape(1, tok),
        member_choice.T,
        group_prob.reshape(1, tok),
        member_score.T,
        norm_gain.reshape(1, dl),
        final_gain.reshape(1, dl),
        w_gate,
        w_up,
        w_down,
    )


def solution(mesh):
    rows = ("grp", "ep")
    placed = (
        P(rows, "tp"),
        P(rows),
        P(rows, None),
        P(rows),
        P(rows, None),
        P("tp"),
        P("ep", "tp", None),
        P("ep", "tp", None),
        P("ep", None, "tp"),
        P("tp"),
    )
    return jax.shard_map(local, mesh=mesh, in_specs=placed, out_specs=P(rows, "tp"), check_vma=False)
```

```python
import functools

import jax
import jax.numpy as jnp
from jax import lax
from jax.experimental import pallas as pl
from jax.experimental.pallas import tpu as pltpu
from jax.sharding import PartitionSpec as P

EPS = 1e-06
F32 = jnp.float32
BF16 = jnp.bfloat16
MESH = pl.DeviceIdType.MESH

CHUNKS = (4, 4, 4, 4)
START = (0, 1, 1, 1)
DIRECT = ()


def dot(a, b):
    return jnp.dot(a, b, preferred_element_type=F32)


def iota(shape, dim):
    return lax.broadcasted_iota(jnp.int32, shape, dim)


def column_of(row, n):
    shape = (n, row.shape[1])
    same = iota(shape, 0) == iota(shape, 1)
    return jnp.sum(jnp.where(same, jnp.broadcast_to(row, shape), 0.0), axis=1, keepdims=True)


def row_of(column, lanes):
    shape = (column.shape[0], lanes)
    same = iota(shape, 0) == iota(shape, 1)
    return jnp.sum(jnp.where(same, jnp.broadcast_to(column, shape), 0.0), axis=0, keepdims=True)


def split3(value):
    first = value.astype(BF16).astype(F32)
    rest = value - first
    second = rest.astype(BF16).astype(F32)
    third = (rest - second).astype(BF16).astype(F32)
    return first, second, third


def kernel(
    dims,
    tokens_hbm,
    group_hbm,
    member_hbm,
    prob_hbm,
    score_hbm,
    gain_hbm,
    final_hbm,
    wg_ref,
    wu_ref,
    wd_ref,
    out_ref,
    tokens_ref,
    group_ref,
    member_ref,
    prob_ref,
    score_ref,
    gain_ref,
    final_ref,
    in_sem,
    wgu,
    wdn,
    sorted_buf,
    meta_src,
    rows_mine,
    rows_other,
    meta_mine,
    meta_other,
    sq_buf,
    sq2_buf,
    rs_send,
    rs_recv,
    hid,
    kept,
    pair_send,
    pair_recv,
    ret_send,
    ret_recv,
    summed_buf,
    w_sem,
    z_send,
    z_recv,
    m_recv,
    r_recv,
    fwd_send,
    fwd_recv,
    mfwd_send,
    mfwd_recv,
    sq_send,
    sq_recv,
    rs_ssem,
    rs_rsem,
    ag_ssem,
    ag_rsem,
    pair_ssem,
    pair_rsem,
    here_z,
    here_x,
    here_c,
):
    n_z, n_x, groups, width = dims
    per_chips = n_z // groups
    tok, dl = tokens_hbm.shape
    cap = tok // groups
    half = n_x // 2
    cols = wgu.shape[2] // 2
    n_chunks = len(CHUNKS)
    bases = [sum(CHUNKS[:c]) for c in range(n_chunks)]
    ep, me = lax.axis_index("ep"), lax.axis_index("tp")
    z, core = lax.div(ep, 2), lax.rem(ep, 2)
    partner = {"ep": 2 * z + 1 - core}
    right = {"tp": lax.rem(me + 1, n_x)}
    left = {"tp": lax.rem(me + n_x - 1, n_x)}

    def at_chip(k):
        return {"ep": 2 * k + core}

    def x_index(offset):
        return lax.rem(me + offset + n_x, n_x)

    def block(index):
        return pl.ds(pl.multiple_of(index * cap, cap), cap)

    def span(c):
        return pl.ds(bases[c] * cap, CHUNKS[c] * cap)

    def n_mine(c):
        return CHUNKS[c] * cap

    def in_chunk(c):
        return (z >= bases[c]) & (z < bases[c] + CHUNKS[c])

    def send(src, dst, ssem, rsem, device):
        pltpu.make_async_remote_copy(
            src_ref=src, dst_ref=dst, send_sem=ssem, recv_sem=rsem, device_id=device, device_id_type=MESH
        ).start()

    def await_bytes(ref, sem):
        pltpu.make_async_copy(ref, ref, sem).wait()

    def signal(sem, device):
        pl.semaphore_signal(sem, inc=1, device_id=device, device_id_type=MESH)

    def each(lo, hi, body):
        def step(i, carry):
            body(i)
            return carry

        lax.fori_loop(lo, hi, step, 0)

    def ranked(index, n, odd):
        moved = jnp.where(index == 0, n - 2, jnp.where(index == n - 1, n - 1, index - 1))
        return jnp.where(odd, moved, index)

    def unranked(rank, n, odd):
        moved = jnp.where(rank == n - 2, 0, jnp.where(rank == n - 1, n - 1, rank + 1))
        return jnp.where(odd, moved, rank)

    def folded(index):
        return jnp.where(index < half, index, n_x - 1 - index + half)

    z_odd, x_odd, c_odd = (me == 0) & (core == 0), (z == 0) & (core == 0), (z == 0) & (me == 0)
    z_rank = ranked(z, n_z, z_odd)
    x_rank = jnp.where(x_odd, lax.rem(folded(me) + n_x - 1, n_x), folded(me))
    c_rank = jnp.where(c_odd, 1 - core, core)

    def z_of(rank):
        return unranked(rank, n_z, z_odd)

    def x_of(rank):
        return folded(jnp.where(x_odd, lax.rem(rank + 1, n_x), rank))

    barrier = pltpu.get_barrier_semaphore()
    each(z_rank + 1, n_z, lambda r: signal(barrier, at_chip(z_of(r))))
    each(x_rank + 1, n_x, lambda r: signal(barrier, {"tp": x_of(r)}))

    @pl.when(c_rank == 0)
    def _():
        signal(barrier, partner)

    smalls = (
        (tokens_hbm, tokens_ref),
        (group_hbm, group_ref),
        (gain_hbm, gain_ref),
        (member_hbm, member_ref),
        (prob_hbm, prob_ref),
        (score_hbm, score_ref),
        (final_hbm, final_ref),
    )
    fetched = [pltpu.make_async_copy(src, dst, in_sem.at[i]) for i, (src, dst) in enumerate(smalls)]
    for fetch in fetched:
        fetch.start()
    loads = []
    for o in range(n_x):
        part = pl.ds(o * cols, cols)
        loads.append(pltpu.make_async_copy(wg_ref.at[0, :, part], wgu.at[o, :, pl.ds(0, cols)], w_sem.at[0]))
        loads.append(pltpu.make_async_copy(wu_ref.at[0, :, part], wgu.at[o, :, pl.ds(cols, cols)], w_sem.at[0]))
    loads.append(pltpu.make_async_copy(wd_ref.at[0], wdn, w_sem.at[1]))
    for load in loads:
        load.start()

    for fetch in fetched:
        fetch.wait()
    values = tokens_ref[...].astype(F32)
    scaled = (values * gain_ref[...]).astype(BF16)
    group_row = group_ref[...]
    chosen = (iota((8, tok), 0) == jnp.broadcast_to(group_row, (8, tok))).astype(F32)
    earlier = (iota((tok, tok), 0) < iota((tok, tok), 1)).astype(F32)
    rank = jnp.sum(dot(chosen, earlier) * chosen, axis=0, keepdims=True)
    slot_row = group_row.astype(F32) * cap + rank
    picker = (iota((tok, tok), 0).astype(F32) == jnp.broadcast_to(slot_row, (tok, tok))).astype(BF16)
    sorted_buf[...] = dot(picker, scaled).astype(BF16)
    square = jnp.sum(values * values, axis=1, keepdims=True)
    sq_buf[pl.ds(me, 1)] = row_of(square, 128).reshape(1, 1, 128)
    rows_mine[block(z), :] = sorted_buf[block(lax.div(z, per_chips)), :]

    def send_rows(k):
        send(sorted_buf.at[block(lax.div(k, per_chips))], rows_mine.at[block(z)], z_send.at[0], z_recv.at[z], at_chip(k))

    def send_meta(k):
        send(meta_src.at[block(lax.div(k, per_chips))], meta_mine.at[block(z)], z_send.at[1], m_recv.at[z], at_chip(k))

    with jax.named_scope("meet"):
        expected = z_rank + x_rank + c_rank

        @pl.when(expected > 0)
        def _():
            pl.semaphore_wait(barrier, expected)

        each(0, z_rank, lambda r: signal(here_z.at[z], at_chip(z_of(r))))
        each(0, x_rank, lambda r: signal(here_x.at[me], {"tp": x_of(r)}))

        @pl.when(c_rank == 1)
        def _():
            signal(here_c, partner)

    def greet(r):
        k = z_of(r)
        pl.semaphore_wait(here_z.at[k], 1)
        send_rows(k)

    with jax.named_scope("greet"):
        each(0, z_rank, lambda r: send_rows(z_of(r)))
        each(z_rank + 1, n_z, greet)

    def send_square(r):
        send(sq_buf.at[me], sq_buf.at[me], sq_send.at[0], sq_recv.at[0], {"tp": x_of(r)})

    def greet_x(r):
        pl.semaphore_wait(here_x.at[x_of(r)], 1)
        send_square(r)

    with jax.named_scope("greet_x"):
        each(0, x_rank, send_square)
        each(x_rank + 1, n_x, greet_x)

        @pl.when(c_rank == 0)
        def _():
            pl.semaphore_wait(here_c, 1)

    def await_blocks(c, ref, sems):
        for k in range(bases[c], bases[c] + CHUNKS[c]):

            @pl.when(z != k)
            def _(k=k):
                await_bytes(ref.at[pl.ds(k * cap, cap)], sems.at[k])

    def take(c):
        await_blocks(c, rows_mine, z_recv)
        send(rows_mine.at[span(c)], rows_other.at[span(c)], fwd_send.at[c], fwd_recv.at[c], partner)

    def make_meta():
        await_bytes(sq_buf.at[pl.ds(0, n_x - 1)], sq_recv.at[0])
        total = jnp.sum(sq_buf[...], axis=0)[:, :tok]
        factor = lax.rsqrt(total / width + EPS)
        score = jnp.exp(score_ref[...])
        weight = prob_ref[...] * score / jnp.sum(score, axis=0, keepdims=True)
        member = iota((8, tok), 0)
        dense = jnp.zeros((8, tok), F32)
        for k in range(member_ref.shape[0]):
            dense = jnp.where(member == member_ref[k : k + 1, :], weight[k : k + 1, :], dense)
        parts = split3(dense)
        factors = split3(factor)
        spread = jnp.zeros((8, tok), F32)
        for k in range(3):
            spread = jnp.where(member == k, factors[k], spread)
        packed = jnp.concatenate([*parts, spread, jnp.zeros((96, tok), F32)], axis=0)
        meta_src[...] = lax.dot_general(
            picker, packed.astype(BF16), (((1,), (1,)), ((), ())), preferred_element_type=F32
        ).astype(BF16)
        meta_mine[block(z), :] = meta_src[block(lax.div(z, per_chips)), :]
        each(0, z_rank, lambda r: send_meta(z_of(r)))
        each(z_rank + 1, n_z, lambda r: send_meta(z_of(r)))

    def pass_meta(c):
        await_blocks(c, meta_mine, m_recv)
        send(meta_mine.at[span(c)], meta_other.at[span(c)], mfwd_send.at[c], mfwd_recv.at[c], partner)

    gate_cols, up_cols = pl.ds(0, cols), pl.ds(cols, cols)

    def partial(c, owner):
        both = jnp.concatenate([rows_mine[span(c), :], rows_other[span(c), :]], axis=0)
        return dot(both, wgu[owner])

    def reduce_ref(buf, c, s, d):
        used = pl.ds(0, 2 * n_mine(c))
        if s > 0:
            return buf.at[c, s, d, used]
        return buf.at[c, s, d, used, up_cols if d == 0 else gate_cols]

    def await_reduce(c, s, d):
        await_bytes(reduce_ref(rs_recv, c, s, d), rs_rsem.at[c, s, d])

    def reduce_send(c, s, d):
        send(
            reduce_ref(rs_send, c, s, d),
            reduce_ref(rs_recv, c, s, d),
            rs_ssem.at[c, s, d],
            rs_rsem.at[c, s, d],
            right if d == 0 else left,
        )

    def reduce_step(c, s):
        n = 2 * n_mine(c)
        if s == 0:
            both = partial(c, x_index(half)).astype(BF16)
            rs_send[c, 0, 0, :n, cols:] = both[:, cols:]
            rs_send[c, 0, 1, :n, :cols] = both[:, :cols]
            reduce_send(c, 0, 0)
            reduce_send(c, 0, 1)
            return
        for d, sign in enumerate((1, -1)):
            mine = partial(c, x_index(sign * (half - s)))
            await_reduce(c, s - 1, d)
            if s == 1:
                lo = d * cols
                alone = slice(lo, lo + cols)
                other = slice(cols - lo, 2 * cols - lo)
                rs_send[c, s, d, :n, alone] = mine[:, alone].astype(BF16)
                rs_send[c, s, d, :n, other] = (mine[:, other] + rs_recv[c, s - 1, d, :n, other].astype(F32)).astype(BF16)
            else:
                rs_send[c, s, d, :n] = (mine + rs_recv[c, s - 1, d, :n].astype(F32)).astype(BF16)
            reduce_send(c, s, d)

    def gather_ref(c, s, d, owner):
        if s < half - 1:
            return hid.at[c, owner, pl.ds(0, 2 * n_mine(c))]
        return hid.at[c, owner, pl.ds(d * n_mine(c), n_mine(c))]

    def gather_all(c):
        for r in range(1, n_x):
            block_me = hid.at[c, me, pl.ds(0, 2 * n_mine(c))]
            send(block_me, block_me, ag_ssem.at[c, 0, 0], ag_rsem.at[c, 0, 0], {"tp": x_index(r)})

    def gather_send(c, s):
        for d, sign in enumerate((1, -1)):
            ref = gather_ref(c, s, d, x_index(-sign * s))
            send(ref, ref, ag_ssem.at[c, s, d], ag_rsem.at[c, s, d], right if d == 0 else left)

    def gather_wait(c, s):
        for d, sign in enumerate((1, -1)):
            await_bytes(gather_ref(c, s, d, x_index(-sign * (s + 1))), ag_rsem.at[c, s, d])

    def info(c):
        return jnp.concatenate([meta_mine[span(c), :], meta_other[span(c), :]], axis=0).astype(F32)

    def activate(c):
        n = 2 * n_mine(c)
        total = partial(c, me)
        await_bytes(meta_other.at[span(c)], mfwd_recv.at[c])
        lane = iota((n, 128), 1)
        factor = jnp.sum(jnp.where(lax.div(lane, 8) == 3, info(c), 0.0), axis=1, keepdims=True)
        for d in range(2):
            await_reduce(c, half - 1, d)
            total = total + rs_recv[c, half - 1, d, :n].astype(F32)
        total = total * factor
        gate, up = total[:, :cols], total[:, cols:]
        hid[c, me, :n] = (gate / (1.0 + jnp.exp(-gate)) * up).astype(BF16)
        if c in DIRECT:
            gather_all(c)
        else:
            gather_send(c, 0)

    def all_others(c):
        return hid.at[c, pl.ds(0, n_x - 1), pl.ds(0, 2 * n_mine(c))]

    def produce(c):
        n = 2 * n_mine(c)
        if c in DIRECT:
            await_bytes(all_others(c), ag_rsem.at[c, 0, 0])
        else:
            gather_wait(c, half - 1)
        hidden = jnp.concatenate([hid[c, o, :n] for o in range(n_x)], axis=1)
        made = dot(hidden, wdn[...])
        lane = iota((n, 128), 1)
        member = 2 * lax.rem(z, per_chips) + core
        named = (lax.rem(lane, 8) == member) & (lane < 24)
        weight = jnp.sum(jnp.where(named, info(c), 0.0), axis=1, keepdims=True)
        made = made.astype(BF16).astype(F32) * weight
        pair_send[span(c), :] = made[n_mine(c) :].astype(BF16)
        send(pair_send.at[span(c)], pair_recv.at[span(c)], pair_ssem.at[c], pair_rsem.at[c], partner)
        kept[span(c), :] = made[: n_mine(c)]

    def give_back(c):
        await_bytes(pair_recv.at[span(c)], pair_rsem.at[c])
        ret_send[span(c), :] = (kept[span(c), :] + pair_recv[span(c), :].astype(F32)).astype(BF16)
        for k in range(bases[c], bases[c] + CHUNKS[c]):

            @pl.when(z == k)
            def _(k=k):
                ret_recv[block(k), :] = ret_send[block(k), :]

            @pl.when(z != k)
            def _(k=k):
                send(ret_send.at[block(k)], ret_recv.at[block(z)], z_send.at[2], r_recv.at[z], at_chip(k))

    def gather_returned():
        for k in range(n_z):

            @pl.when(z != k)
            def _(k=k):
                await_bytes(ret_recv.at[block(k)], r_recv.at[k])

        row = iota((n_z * cap, tok), 0)
        slots = lax.div(row, per_chips * cap) * cap + lax.rem(row, cap)
        unpick = (slots.astype(F32) == jnp.broadcast_to(slot_row, row.shape)).astype(BF16)
        moe = lax.dot_general(unpick, ret_recv[...], (((0,), (0,)), ((), ())), preferred_element_type=F32)
        summed = tokens_ref[...].astype(F32) + moe
        summed_buf[...] = summed
        total = jnp.sum(summed * summed, axis=1, keepdims=True)
        sq2_buf[pl.ds(me, 1)] = row_of(total, 128).reshape(1, 1, 128)

        def send_total(r):
            send(sq2_buf.at[me], sq2_buf.at[me], sq_send.at[1], sq_recv.at[1], {"tp": r})

        each(0, me, send_total)
        each(me + 1, n_x, send_total)

    def write_out():
        await_bytes(sq2_buf.at[pl.ds(0, n_x - 1)], sq_recv.at[1])
        total = column_of(jnp.sum(sq2_buf[...], axis=0), tok)
        out_ref[...] = (summed_buf[...] * lax.rsqrt(total / width + EPS) * final_ref[...]).astype(BF16)

    def stage(c, k):
        if k == 0:
            await_bytes(rows_other.at[span(c)], fwd_recv.at[c])
            reduce_step(c, 0)
        elif k < half:
            reduce_step(c, k)
            if k == half - 2:
                pass_meta(c)
        elif k == half:
            activate(c)
        elif c in DIRECT:
            (produce if k == half + 1 else give_back)(c)
        elif k < 2 * half:
            gather_wait(c, k - half - 1)
            gather_send(c, k - half)
        elif k == 2 * half:
            produce(c)
        else:
            give_back(c)

    ends = [half + 2 if c in DIRECT else 2 * half + 1 for c in range(n_chunks)]
    total_steps = max(START[c] + ends[c] for c in range(n_chunks)) + 1
    for c in range(n_chunks):
        if START[c] == 0:
            with jax.named_scope(f"take#c={c}"):
                take(c)
    with jax.named_scope("weights"):
        await_bytes(wgu, w_sem.at[0])
        await_bytes(wdn, w_sem.at[1])
    for t in range(total_steps):
        for c in range(n_chunks):
            k = t - START[c]
            if 0 <= k <= ends[c]:
                with jax.named_scope(f"stage#c={c}#k={k}"):
                    stage(c, k)
            if k == -1:
                with jax.named_scope(f"take#c={c}"):
                    take(c)
        if t == 1:
            with jax.named_scope("make_meta"):
                make_meta()
    with jax.named_scope("returned"):
        gather_returned()
    with jax.named_scope("write"):
        write_out()

    n_remote = cap * (n_z - 1)
    flat = wdn.at[pl.ds(0, n_remote)]
    await_bytes(flat, z_send.at[0])
    await_bytes(wdn.at[pl.ds(0, n_remote), pl.ds(0, 128)], z_send.at[1])
    await_bytes(flat, z_send.at[2])
    await_bytes(sq_buf.at[pl.ds(0, n_x - 1)], sq_send.at[0])
    await_bytes(sq_buf.at[pl.ds(0, n_x - 1)], sq_send.at[1])
    for c in range(n_chunks):
        await_bytes(rows_mine.at[span(c)], fwd_send.at[c])
        await_bytes(meta_mine.at[span(c)], mfwd_send.at[c])
        await_bytes(pair_recv.at[span(c)], pair_ssem.at[c])
        if c in DIRECT:
            await_bytes(all_others(c), ag_ssem.at[c, 0, 0])
        for s in range(half):
            for d in range(2):
                await_bytes(reduce_ref(rs_send, c, s, d), rs_ssem.at[c, s, d])
                if c not in DIRECT:
                    await_bytes(gather_ref(c, s, d, me), ag_ssem.at[c, s, d])


def local(tokens, group_choice, member_choice, group_prob, member_score, norm_gain, w_gate, w_up, w_down, final_gain):
    n_z, n_x = lax.axis_size("ep") // 2, lax.axis_size("tp")
    groups = max(2, 2 * n_z // 8)
    tok, dl = tokens.shape
    top = member_choice.shape[1]
    ff = w_gate.shape[2]
    cap = tok // groups
    cols = ff // n_x
    n_chunks = len(CHUNKS)
    n_rows = 2 * cap * max(CHUNKS)
    n_all = n_z * cap
    half = n_x // 2
    dma = pltpu.SemaphoreType.DMA
    vmem = pl.BlockSpec(memory_space=pltpu.VMEM)
    hbm = pl.BlockSpec(memory_space=pl.ANY)
    return pl.pallas_call(
        functools.partial(kernel, (n_z, n_x, groups, dl * n_x)),
        out_shape=jax.ShapeDtypeStruct((tok, dl), BF16),
        in_specs=[hbm] * 10,
        out_specs=vmem,
        scratch_shapes=[
            pltpu.VMEM((tok, dl), BF16),
            pltpu.VMEM((1, tok), jnp.int32),
            pltpu.VMEM((top, tok), jnp.int32),
            pltpu.VMEM((1, tok), F32),
            pltpu.VMEM((top, tok), F32),
            pltpu.VMEM((1, dl), F32),
            pltpu.VMEM((1, dl), F32),
            dma((7,)),
            pltpu.VMEM((n_x, dl, 2 * cols), BF16),
            pltpu.VMEM((ff, dl), BF16),
            pltpu.VMEM((tok, dl), BF16),
            pltpu.VMEM((tok, 128), BF16),
            pltpu.VMEM((n_all, dl), BF16),
            pltpu.VMEM((n_all, dl), BF16),
            pltpu.VMEM((n_all, 128), BF16),
            pltpu.VMEM((n_all, 128), BF16),
            pltpu.VMEM((n_x, 1, 128), F32),
            pltpu.VMEM((n_x, 1, 128), F32),
            pltpu.VMEM((n_chunks, half, 2, n_rows, 2 * cols), BF16),
            pltpu.VMEM((n_chunks, half, 2, n_rows, 2 * cols), BF16),
            pltpu.VMEM((n_chunks, n_x, n_rows, cols), BF16),
            pltpu.VMEM((n_all, dl), F32),
            pltpu.VMEM((n_all, dl), BF16),
            pltpu.VMEM((n_all, dl), BF16),
            pltpu.VMEM((n_all, dl), BF16),
            pltpu.VMEM((n_all, dl), BF16),
            pltpu.VMEM((tok, dl), F32),
            dma((2,)),
            dma((3,)),
            dma((n_z,)),
            dma((n_z,)),
            dma((n_z,)),
            dma((n_chunks,)),
            dma((n_chunks,)),
            dma((n_chunks,)),
            dma((n_chunks,)),
            dma((2,)),
            dma((2,)),
            dma((n_chunks, half, 2)),
            dma((n_chunks, half, 2)),
            dma((n_chunks, half, 2)),
            dma((n_chunks, half, 2)),
            dma((n_chunks,)),
            dma((n_chunks,)),
            pltpu.SemaphoreType.REGULAR((n_z,)),
            pltpu.SemaphoreType.REGULAR((n_x,)),
            pltpu.SemaphoreType.REGULAR,
        ],
        compiler_params=pltpu.CompilerParams(
            collective_id=0, has_side_effects=True, vmem_limit_bytes=67043328
        ),
    )(
        tokens,
        group_choice.reshape(1, tok),
        member_choice.T,
        group_prob.reshape(1, tok),
        member_score.T,
        norm_gain.reshape(1, dl),
        final_gain.reshape(1, dl),
        w_gate,
        w_up,
        w_down,
    )


def solution(mesh):
    rows = ("grp", "ep")
    placed = (
        P(rows, "tp"),
        P(rows),
        P(rows, None),
        P(rows),
        P(rows, None),
        P("tp"),
        P("ep", "tp", None),
        P("ep", "tp", None),
        P("ep", None, "tp"),
        P("tp"),
    )
    return jax.shard_map(local, mesh=mesh, in_specs=placed, out_specs=P(rows, "tp"), check_vma=False)
```

```python
import functools

import jax
import jax.numpy as jnp
from jax import lax
from jax.experimental import pallas as pl
from jax.experimental.pallas import tpu as pltpu
from jax.sharding import PartitionSpec as P

EPS = 1e-06
F32 = jnp.float32
BF16 = jnp.bfloat16
MESH = pl.DeviceIdType.MESH

CHUNKS = (4, 4, 4, 4)
ORDER = (0, 3, 1, 2)
START = (0, 2, 2, 1)
DIRECT = ()


def dot(a, b):
    return jnp.dot(a, b, preferred_element_type=F32)


def iota(shape, dim):
    return lax.broadcasted_iota(jnp.int32, shape, dim)


def column_of(row, n):
    shape = (n, row.shape[1])
    same = iota(shape, 0) == iota(shape, 1)
    return jnp.sum(jnp.where(same, jnp.broadcast_to(row, shape), 0.0), axis=1, keepdims=True)


def row_of(column, lanes):
    shape = (column.shape[0], lanes)
    same = iota(shape, 0) == iota(shape, 1)
    return jnp.sum(jnp.where(same, jnp.broadcast_to(column, shape), 0.0), axis=0, keepdims=True)


def split3(value):
    first = value.astype(BF16).astype(F32)
    rest = value - first
    second = rest.astype(BF16).astype(F32)
    third = (rest - second).astype(BF16).astype(F32)
    return first, second, third


def kernel(
    dims,
    tokens_hbm,
    group_hbm,
    member_hbm,
    prob_hbm,
    score_hbm,
    gain_hbm,
    final_hbm,
    wg_ref,
    wu_ref,
    wd_ref,
    out_ref,
    tokens_ref,
    group_ref,
    member_ref,
    prob_ref,
    score_ref,
    gain_ref,
    final_ref,
    in_sem,
    wgu,
    wdn,
    sorted_buf,
    meta_src,
    rows_mine,
    rows_other,
    meta_mine,
    meta_other,
    sq_buf,
    sq2_buf,
    rs_send,
    rs_recv,
    hid,
    kept,
    pair_send,
    pair_recv,
    ret_send,
    ret_recv,
    summed_buf,
    w_sem,
    z_send,
    z_recv,
    m_recv,
    r_recv,
    fwd_send,
    fwd_recv,
    mfwd_send,
    mfwd_recv,
    sq_send,
    sq_recv,
    rs_ssem,
    rs_rsem,
    ag_ssem,
    ag_rsem,
    pair_ssem,
    pair_rsem,
    here_z,
    here_x,
    here_c,
):
    n_z, n_x, groups, width = dims
    per_chips = n_z // groups
    tok, dl = tokens_hbm.shape
    cap = tok // groups
    half = n_x // 2
    cols = wgu.shape[2] // 2
    n_chunks = len(CHUNKS)
    bases = [sum(CHUNKS[:c]) for c in range(n_chunks)]
    ep, me = lax.axis_index("ep"), lax.axis_index("tp")
    z, core = lax.div(ep, 2), lax.rem(ep, 2)
    partner = {"ep": 2 * z + 1 - core}
    right = {"tp": lax.rem(me + 1, n_x)}
    left = {"tp": lax.rem(me + n_x - 1, n_x)}

    def at_chip(k):
        return {"ep": 2 * k + core}

    def x_index(offset):
        return lax.rem(me + offset + n_x, n_x)

    def block(index):
        return pl.ds(pl.multiple_of(index * cap, cap), cap)

    def span(c):
        return pl.ds(bases[c] * cap, CHUNKS[c] * cap)

    def n_mine(c):
        return CHUNKS[c] * cap

    def in_chunk(c):
        return (z >= bases[c]) & (z < bases[c] + CHUNKS[c])

    def send(src, dst, ssem, rsem, device):
        pltpu.make_async_remote_copy(
            src_ref=src, dst_ref=dst, send_sem=ssem, recv_sem=rsem, device_id=device, device_id_type=MESH
        ).start()

    def await_bytes(ref, sem):
        pltpu.make_async_copy(ref, ref, sem).wait()

    def signal(sem, device):
        pl.semaphore_signal(sem, inc=1, device_id=device, device_id_type=MESH)

    def each(lo, hi, body):
        def step(i, carry):
            body(i)
            return carry

        lax.fori_loop(lo, hi, step, 0)

    def ranked(index, n, odd):
        moved = jnp.where(index == 0, n - 2, jnp.where(index == n - 1, n - 1, index - 1))
        return jnp.where(odd, moved, index)

    def unranked(rank, n, odd):
        moved = jnp.where(rank == n - 2, 0, jnp.where(rank == n - 1, n - 1, rank + 1))
        return jnp.where(odd, moved, rank)

    def folded(index):
        return jnp.where(index < half, index, n_x - 1 - index + half)

    z_odd, x_odd, c_odd = (me == 0) & (core == 0), (z == 0) & (core == 0), (z == 0) & (me == 0)
    z_rank = ranked(z, n_z, z_odd)
    x_rank = jnp.where(x_odd, lax.rem(folded(me) + n_x - 1, n_x), folded(me))
    c_rank = jnp.where(c_odd, 1 - core, core)

    def z_of(rank):
        return unranked(rank, n_z, z_odd)

    def x_of(rank):
        return folded(jnp.where(x_odd, lax.rem(rank + 1, n_x), rank))

    barrier = pltpu.get_barrier_semaphore()
    each(z_rank + 1, n_z, lambda r: signal(barrier, at_chip(z_of(r))))
    each(x_rank + 1, n_x, lambda r: signal(barrier, {"tp": x_of(r)}))

    @pl.when(c_rank == 0)
    def _():
        signal(barrier, partner)

    smalls = (
        (tokens_hbm, tokens_ref),
        (group_hbm, group_ref),
        (gain_hbm, gain_ref),
        (member_hbm, member_ref),
        (prob_hbm, prob_ref),
        (score_hbm, score_ref),
        (final_hbm, final_ref),
    )
    fetched = [pltpu.make_async_copy(src, dst, in_sem.at[i]) for i, (src, dst) in enumerate(smalls)]
    for fetch in fetched:
        fetch.start()
    loads = []
    for o in range(n_x):
        part = pl.ds(o * cols, cols)
        loads.append(pltpu.make_async_copy(wg_ref.at[0, :, part], wgu.at[o, :, pl.ds(0, cols)], w_sem.at[0]))
        loads.append(pltpu.make_async_copy(wu_ref.at[0, :, part], wgu.at[o, :, pl.ds(cols, cols)], w_sem.at[0]))
    loads.append(pltpu.make_async_copy(wd_ref.at[0], wdn, w_sem.at[1]))
    for load in loads:
        load.start()

    for fetch in fetched:
        fetch.wait()
    values = tokens_ref[...].astype(F32)
    scaled = (values * gain_ref[...]).astype(BF16)
    group_row = group_ref[...]
    chosen = (iota((8, tok), 0) == jnp.broadcast_to(group_row, (8, tok))).astype(F32)
    earlier = (iota((tok, tok), 0) < iota((tok, tok), 1)).astype(F32)
    rank = jnp.sum(dot(chosen, earlier) * chosen, axis=0, keepdims=True)
    slot_row = group_row.astype(F32) * cap + rank
    picker = (iota((tok, tok), 0).astype(F32) == jnp.broadcast_to(slot_row, (tok, tok))).astype(BF16)
    sorted_buf[...] = dot(picker, scaled).astype(BF16)
    square = jnp.sum(values * values, axis=1, keepdims=True)
    sq_buf[pl.ds(me, 1)] = row_of(square, 128).reshape(1, 1, 128)
    rows_mine[block(z), :] = sorted_buf[block(lax.div(z, per_chips)), :]

    def send_rows(k):
        send(sorted_buf.at[block(lax.div(k, per_chips))], rows_mine.at[block(z)], z_send.at[0], z_recv.at[z], at_chip(k))

    def send_meta(k):
        send(meta_src.at[block(lax.div(k, per_chips))], meta_mine.at[block(z)], z_send.at[1], m_recv.at[z], at_chip(k))

    with jax.named_scope("meet"):
        expected = z_rank + x_rank + c_rank

        @pl.when(expected > 0)
        def _():
            pl.semaphore_wait(barrier, expected)

        each(0, z_rank, lambda r: signal(here_z.at[z], at_chip(z_of(r))))
        each(0, x_rank, lambda r: signal(here_x.at[me], {"tp": x_of(r)}))

        @pl.when(c_rank == 1)
        def _():
            signal(here_c, partner)

    def greet(r):
        k = z_of(r)
        pl.semaphore_wait(here_z.at[k], 1)
        send_rows(k)

    with jax.named_scope("greet"):
        each(0, z_rank, lambda r: send_rows(z_of(r)))
        each(z_rank + 1, n_z, greet)

    def send_square(r):
        send(sq_buf.at[me], sq_buf.at[me], sq_send.at[0], sq_recv.at[0], {"tp": x_of(r)})

    def greet_x(r):
        pl.semaphore_wait(here_x.at[x_of(r)], 1)
        send_square(r)

    with jax.named_scope("greet_x"):
        each(0, x_rank, send_square)
        each(x_rank + 1, n_x, greet_x)

        @pl.when(c_rank == 0)
        def _():
            pl.semaphore_wait(here_c, 1)

    def await_blocks(c, ref, sems):
        for k in range(bases[c], bases[c] + CHUNKS[c]):

            @pl.when(z != k)
            def _(k=k):
                await_bytes(ref.at[pl.ds(k * cap, cap)], sems.at[k])

    def take(c):
        await_blocks(c, rows_mine, z_recv)
        send(rows_mine.at[span(c)], rows_other.at[span(c)], fwd_send.at[c], fwd_recv.at[c], partner)

    def make_meta():
        await_bytes(sq_buf.at[pl.ds(0, n_x - 1)], sq_recv.at[0])
        total = jnp.sum(sq_buf[...], axis=0)[:, :tok]
        factor = lax.rsqrt(total / width + EPS)
        score = jnp.exp(score_ref[...])
        weight = prob_ref[...] * score / jnp.sum(score, axis=0, keepdims=True)
        member = iota((8, tok), 0)
        dense = jnp.zeros((8, tok), F32)
        for k in range(member_ref.shape[0]):
            dense = jnp.where(member == member_ref[k : k + 1, :], weight[k : k + 1, :], dense)
        parts = split3(dense)
        factors = split3(factor)
        spread = jnp.zeros((8, tok), F32)
        for k in range(3):
            spread = jnp.where(member == k, factors[k], spread)
        packed = jnp.concatenate([*parts, spread, jnp.zeros((96, tok), F32)], axis=0)
        meta_src[...] = lax.dot_general(
            picker, packed.astype(BF16), (((1,), (1,)), ((), ())), preferred_element_type=F32
        ).astype(BF16)
        meta_mine[block(z), :] = meta_src[block(lax.div(z, per_chips)), :]
        each(0, z_rank, lambda r: send_meta(z_of(r)))
        each(z_rank + 1, n_z, lambda r: send_meta(z_of(r)))

    def pass_meta(c):
        await_blocks(c, meta_mine, m_recv)
        send(meta_mine.at[span(c)], meta_other.at[span(c)], mfwd_send.at[c], mfwd_recv.at[c], partner)

    gate_cols, up_cols = pl.ds(0, cols), pl.ds(cols, cols)

    def partial(c, owner):
        both = jnp.concatenate([rows_mine[span(c), :], rows_other[span(c), :]], axis=0)
        return dot(both, wgu[owner])

    def reduce_ref(buf, c, s, d):
        used = pl.ds(0, 2 * n_mine(c))
        if s > 0:
            return buf.at[c, s, d, used]
        return buf.at[c, s, d, used, up_cols if d == 0 else gate_cols]

    def await_reduce(c, s, d):
        await_bytes(reduce_ref(rs_recv, c, s, d), rs_rsem.at[c, s, d])

    def reduce_send(c, s, d):
        send(
            reduce_ref(rs_send, c, s, d),
            reduce_ref(rs_recv, c, s, d),
            rs_ssem.at[c, s, d],
            rs_rsem.at[c, s, d],
            right if d == 0 else left,
        )

    def reduce_step(c, s):
        n = 2 * n_mine(c)
        if s == 0:
            both = partial(c, x_index(half)).astype(BF16)
            rs_send[c, 0, 0, :n, cols:] = both[:, cols:]
            rs_send[c, 0, 1, :n, :cols] = both[:, :cols]
            reduce_send(c, 0, 0)
            reduce_send(c, 0, 1)
            return
        for d, sign in enumerate((1, -1)):
            mine = partial(c, x_index(sign * (half - s)))
            await_reduce(c, s - 1, d)
            if s == 1:
                lo = d * cols
                alone = slice(lo, lo + cols)
                other = slice(cols - lo, 2 * cols - lo)
                rs_send[c, s, d, :n, alone] = mine[:, alone].astype(BF16)
                rs_send[c, s, d, :n, other] = (mine[:, other] + rs_recv[c, s - 1, d, :n, other].astype(F32)).astype(BF16)
            else:
                rs_send[c, s, d, :n] = (mine + rs_recv[c, s - 1, d, :n].astype(F32)).astype(BF16)
            reduce_send(c, s, d)

    def gather_ref(c, s, d, owner):
        if s < half - 1:
            return hid.at[c, owner, pl.ds(0, 2 * n_mine(c))]
        return hid.at[c, owner, pl.ds(d * n_mine(c), n_mine(c))]

    def gather_all(c):
        for r in range(1, n_x):
            block_me = hid.at[c, me, pl.ds(0, 2 * n_mine(c))]
            send(block_me, block_me, ag_ssem.at[c, 0, 0], ag_rsem.at[c, 0, 0], {"tp": x_index(r)})

    def gather_send(c, s):
        for d, sign in enumerate((1, -1)):
            ref = gather_ref(c, s, d, x_index(-sign * s))
            send(ref, ref, ag_ssem.at[c, s, d], ag_rsem.at[c, s, d], right if d == 0 else left)

    def gather_wait(c, s):
        for d, sign in enumerate((1, -1)):
            await_bytes(gather_ref(c, s, d, x_index(-sign * (s + 1))), ag_rsem.at[c, s, d])

    def info(c):
        return jnp.concatenate([meta_mine[span(c), :], meta_other[span(c), :]], axis=0).astype(F32)

    def activate(c):
        n = 2 * n_mine(c)
        total = partial(c, me)
        await_bytes(meta_other.at[span(c)], mfwd_recv.at[c])
        lane = iota((n, 128), 1)
        factor = jnp.sum(jnp.where(lax.div(lane, 8) == 3, info(c), 0.0), axis=1, keepdims=True)
        for d in range(2):
            await_reduce(c, half - 1, d)
            total = total + rs_recv[c, half - 1, d, :n].astype(F32)
        total = total * factor
        gate, up = total[:, :cols], total[:, cols:]
        hid[c, me, :n] = (gate / (1.0 + jnp.exp(-gate)) * up).astype(BF16)
        if c in DIRECT:
            gather_all(c)
        else:
            gather_send(c, 0)

    def all_others(c):
        return hid.at[c, pl.ds(0, n_x - 1), pl.ds(0, 2 * n_mine(c))]

    def produce(c):
        n = 2 * n_mine(c)
        if c in DIRECT:
            await_bytes(all_others(c), ag_rsem.at[c, 0, 0])
        else:
            gather_wait(c, half - 1)
        hidden = jnp.concatenate([hid[c, o, :n] for o in range(n_x)], axis=1)
        made = dot(hidden, wdn[...])
        lane = iota((n, 128), 1)
        member = 2 * lax.rem(z, per_chips) + core
        named = (lax.rem(lane, 8) == member) & (lane < 24)
        weight = jnp.sum(jnp.where(named, info(c), 0.0), axis=1, keepdims=True)
        made = made.astype(BF16).astype(F32) * weight
        pair_send[span(c), :] = made[n_mine(c) :].astype(BF16)
        send(pair_send.at[span(c)], pair_recv.at[span(c)], pair_ssem.at[c], pair_rsem.at[c], partner)
        kept[span(c), :] = made[: n_mine(c)]

    def give_back(c):
        await_bytes(pair_recv.at[span(c)], pair_rsem.at[c])
        ret_send[span(c), :] = (kept[span(c), :] + pair_recv[span(c), :].astype(F32)).astype(BF16)
        for k in range(bases[c], bases[c] + CHUNKS[c]):

            @pl.when(z == k)
            def _(k=k):
                ret_recv[block(k), :] = ret_send[block(k), :]

            @pl.when(z != k)
            def _(k=k):
                send(ret_send.at[block(k)], ret_recv.at[block(z)], z_send.at[2], r_recv.at[z], at_chip(k))

    def gather_returned():
        for k in range(n_z):

            @pl.when(z != k)
            def _(k=k):
                await_bytes(ret_recv.at[block(k)], r_recv.at[k])

        row = iota((n_z * cap, tok), 0)
        slots = lax.div(row, per_chips * cap) * cap + lax.rem(row, cap)
        unpick = (slots.astype(F32) == jnp.broadcast_to(slot_row, row.shape)).astype(BF16)
        moe = lax.dot_general(unpick, ret_recv[...], (((0,), (0,)), ((), ())), preferred_element_type=F32)
        summed = tokens_ref[...].astype(F32) + moe
        summed_buf[...] = summed
        total = jnp.sum(summed * summed, axis=1, keepdims=True)
        sq2_buf[pl.ds(me, 1)] = row_of(total, 128).reshape(1, 1, 128)

        def send_total(r):
            send(sq2_buf.at[me], sq2_buf.at[me], sq_send.at[1], sq_recv.at[1], {"tp": r})

        each(0, me, send_total)
        each(me + 1, n_x, send_total)

    def write_out():
        await_bytes(sq2_buf.at[pl.ds(0, n_x - 1)], sq_recv.at[1])
        total = column_of(jnp.sum(sq2_buf[...], axis=0), tok)
        out_ref[...] = (summed_buf[...] * lax.rsqrt(total / width + EPS) * final_ref[...]).astype(BF16)

    def stage(c, k):
        if k == 0:
            await_bytes(rows_other.at[span(c)], fwd_recv.at[c])
            reduce_step(c, 0)
        elif k < half:
            reduce_step(c, k)
            if k == half - 2:
                pass_meta(c)
        elif k == half:
            activate(c)
        elif c in DIRECT:
            (produce if k == half + 1 else give_back)(c)
        elif k < 2 * half:
            gather_wait(c, k - half - 1)
            gather_send(c, k - half)
        elif k == 2 * half:
            produce(c)
        else:
            give_back(c)

    ends = [half + 2 if c in DIRECT else 2 * half + 1 for c in range(n_chunks)]
    total_steps = max(START[c] + ends[c] for c in range(n_chunks)) + 1
    for c in ORDER:
        if START[c] == 0:
            with jax.named_scope(f"take#c={c}"):
                take(c)
    with jax.named_scope("weights"):
        await_bytes(wgu, w_sem.at[0])
        await_bytes(wdn, w_sem.at[1])
    for t in range(total_steps):
        for c in ORDER:
            k = t - START[c]
            if 0 <= k <= ends[c]:
                with jax.named_scope(f"stage#c={c}#k={k}"):
                    stage(c, k)
        if t == 1:
            with jax.named_scope("make_meta"):
                make_meta()
        for c in ORDER:
            if t == START[c] - 1:
                with jax.named_scope(f"take#c={c}"):
                    take(c)
    with jax.named_scope("returned"):
        gather_returned()
    with jax.named_scope("write"):
        write_out()

    n_remote = cap * (n_z - 1)
    flat = wdn.at[pl.ds(0, n_remote)]
    await_bytes(flat, z_send.at[0])
    await_bytes(wdn.at[pl.ds(0, n_remote), pl.ds(0, 128)], z_send.at[1])
    await_bytes(flat, z_send.at[2])
    await_bytes(sq_buf.at[pl.ds(0, n_x - 1)], sq_send.at[0])
    await_bytes(sq_buf.at[pl.ds(0, n_x - 1)], sq_send.at[1])
    for c in range(n_chunks):
        await_bytes(rows_mine.at[span(c)], fwd_send.at[c])
        await_bytes(meta_mine.at[span(c)], mfwd_send.at[c])
        await_bytes(pair_recv.at[span(c)], pair_ssem.at[c])
        if c in DIRECT:
            await_bytes(all_others(c), ag_ssem.at[c, 0, 0])
        for s in range(half):
            for d in range(2):
                await_bytes(reduce_ref(rs_send, c, s, d), rs_ssem.at[c, s, d])
                if c not in DIRECT:
                    await_bytes(gather_ref(c, s, d, me), ag_ssem.at[c, s, d])


def local(tokens, group_choice, member_choice, group_prob, member_score, norm_gain, w_gate, w_up, w_down, final_gain):
    n_z, n_x = lax.axis_size("ep") // 2, lax.axis_size("tp")
    groups = max(2, 2 * n_z // 8)
    tok, dl = tokens.shape
    top = member_choice.shape[1]
    ff = w_gate.shape[2]
    cap = tok // groups
    cols = ff // n_x
    n_chunks = len(CHUNKS)
    n_rows = 2 * cap * max(CHUNKS)
    n_all = n_z * cap
    half = n_x // 2
    dma = pltpu.SemaphoreType.DMA
    vmem = pl.BlockSpec(memory_space=pltpu.VMEM)
    hbm = pl.BlockSpec(memory_space=pl.ANY)
    return pl.pallas_call(
        functools.partial(kernel, (n_z, n_x, groups, dl * n_x)),
        out_shape=jax.ShapeDtypeStruct((tok, dl), BF16),
        in_specs=[hbm] * 10,
        out_specs=vmem,
        scratch_shapes=[
            pltpu.VMEM((tok, dl), BF16),
            pltpu.VMEM((1, tok), jnp.int32),
            pltpu.VMEM((top, tok), jnp.int32),
            pltpu.VMEM((1, tok), F32),
            pltpu.VMEM((top, tok), F32),
            pltpu.VMEM((1, dl), F32),
            pltpu.VMEM((1, dl), F32),
            dma((7,)),
            pltpu.VMEM((n_x, dl, 2 * cols), BF16),
            pltpu.VMEM((ff, dl), BF16),
            pltpu.VMEM((tok, dl), BF16),
            pltpu.VMEM((tok, 128), BF16),
            pltpu.VMEM((n_all, dl), BF16),
            pltpu.VMEM((n_all, dl), BF16),
            pltpu.VMEM((n_all, 128), BF16),
            pltpu.VMEM((n_all, 128), BF16),
            pltpu.VMEM((n_x, 1, 128), F32),
            pltpu.VMEM((n_x, 1, 128), F32),
            pltpu.VMEM((n_chunks, half, 2, n_rows, 2 * cols), BF16),
            pltpu.VMEM((n_chunks, half, 2, n_rows, 2 * cols), BF16),
            pltpu.VMEM((n_chunks, n_x, n_rows, cols), BF16),
            pltpu.VMEM((n_all, dl), F32),
            pltpu.VMEM((n_all, dl), BF16),
            pltpu.VMEM((n_all, dl), BF16),
            pltpu.VMEM((n_all, dl), BF16),
            pltpu.VMEM((n_all, dl), BF16),
            pltpu.VMEM((tok, dl), F32),
            dma((2,)),
            dma((3,)),
            dma((n_z,)),
            dma((n_z,)),
            dma((n_z,)),
            dma((n_chunks,)),
            dma((n_chunks,)),
            dma((n_chunks,)),
            dma((n_chunks,)),
            dma((2,)),
            dma((2,)),
            dma((n_chunks, half, 2)),
            dma((n_chunks, half, 2)),
            dma((n_chunks, half, 2)),
            dma((n_chunks, half, 2)),
            dma((n_chunks,)),
            dma((n_chunks,)),
            pltpu.SemaphoreType.REGULAR((n_z,)),
            pltpu.SemaphoreType.REGULAR((n_x,)),
            pltpu.SemaphoreType.REGULAR,
        ],
        compiler_params=pltpu.CompilerParams(
            collective_id=0, has_side_effects=True, vmem_limit_bytes=67043328
        ),
    )(
        tokens,
        group_choice.reshape(1, tok),
        member_choice.T,
        group_prob.reshape(1, tok),
        member_score.T,
        norm_gain.reshape(1, dl),
        final_gain.reshape(1, dl),
        w_gate,
        w_up,
        w_down,
    )


def solution(mesh):
    rows = ("grp", "ep")
    placed = (
        P(rows, "tp"),
        P(rows),
        P(rows, None),
        P(rows),
        P(rows, None),
        P("tp"),
        P("ep", "tp", None),
        P("ep", "tp", None),
        P("ep", None, "tp"),
        P("tp"),
    )
    return jax.shard_map(local, mesh=mesh, in_specs=placed, out_specs=P(rows, "tp"), check_vma=False)
```

```python
import functools

import jax
import jax.numpy as jnp
from jax import lax
from jax.experimental import pallas as pl
from jax.experimental.pallas import tpu as pltpu
from jax.sharding import PartitionSpec as P

EPS = 1e-06
F32 = jnp.float32
BF16 = jnp.bfloat16
MESH = pl.DeviceIdType.MESH

CHUNKS = (4, 4, 4, 4)
ORDER = (0, 3, 2, 1)
START = (0, 2, 2, 1)
DIRECT = ()


def dot(a, b):
    return jnp.dot(a, b, preferred_element_type=F32)


def iota(shape, dim):
    return lax.broadcasted_iota(jnp.int32, shape, dim)


def column_of(row, n):
    shape = (n, row.shape[1])
    same = iota(shape, 0) == iota(shape, 1)
    return jnp.sum(jnp.where(same, jnp.broadcast_to(row, shape), 0.0), axis=1, keepdims=True)


def row_of(column, lanes):
    shape = (column.shape[0], lanes)
    same = iota(shape, 0) == iota(shape, 1)
    return jnp.sum(jnp.where(same, jnp.broadcast_to(column, shape), 0.0), axis=0, keepdims=True)


def split3(value):
    first = value.astype(BF16).astype(F32)
    rest = value - first
    second = rest.astype(BF16).astype(F32)
    third = (rest - second).astype(BF16).astype(F32)
    return first, second, third


def kernel(
    dims,
    tokens_hbm,
    group_hbm,
    member_hbm,
    prob_hbm,
    score_hbm,
    gain_hbm,
    final_hbm,
    wg_ref,
    wu_ref,
    wd_ref,
    out_ref,
    tokens_ref,
    group_ref,
    member_ref,
    prob_ref,
    score_ref,
    gain_ref,
    final_ref,
    in_sem,
    wgu,
    wdn,
    sorted_buf,
    meta_src,
    rows_mine,
    rows_other,
    meta_mine,
    meta_other,
    sq_buf,
    sq2_buf,
    rs_send,
    rs_recv,
    hid,
    kept,
    pair_send,
    pair_recv,
    ret_send,
    ret_recv,
    summed_buf,
    w_sem,
    z_send,
    z_recv,
    m_recv,
    r_recv,
    fwd_send,
    fwd_recv,
    mfwd_send,
    mfwd_recv,
    sq_send,
    sq_recv,
    rs_ssem,
    rs_rsem,
    ag_ssem,
    ag_rsem,
    pair_ssem,
    pair_rsem,
    here_z,
    here_x,
    here_c,
):
    n_z, n_x, groups, width = dims
    per_chips = n_z // groups
    tok, dl = tokens_hbm.shape
    cap = tok // groups
    half = n_x // 2
    cols = wgu.shape[2] // 2
    n_chunks = len(CHUNKS)
    bases = [sum(CHUNKS[:c]) for c in range(n_chunks)]
    ep, me = lax.axis_index("ep"), lax.axis_index("tp")
    z, core = lax.div(ep, 2), lax.rem(ep, 2)
    partner = {"ep": 2 * z + 1 - core}
    right = {"tp": lax.rem(me + 1, n_x)}
    left = {"tp": lax.rem(me + n_x - 1, n_x)}

    def at_chip(k):
        return {"ep": 2 * k + core}

    def x_index(offset):
        return lax.rem(me + offset + n_x, n_x)

    def block(index):
        return pl.ds(pl.multiple_of(index * cap, cap), cap)

    def span(c):
        return pl.ds(bases[c] * cap, CHUNKS[c] * cap)

    def n_mine(c):
        return CHUNKS[c] * cap

    def in_chunk(c):
        return (z >= bases[c]) & (z < bases[c] + CHUNKS[c])

    def send(src, dst, ssem, rsem, device):
        pltpu.make_async_remote_copy(
            src_ref=src, dst_ref=dst, send_sem=ssem, recv_sem=rsem, device_id=device, device_id_type=MESH
        ).start()

    def await_bytes(ref, sem):
        pltpu.make_async_copy(ref, ref, sem).wait()

    def signal(sem, device):
        pl.semaphore_signal(sem, inc=1, device_id=device, device_id_type=MESH)

    def each(lo, hi, body):
        def step(i, carry):
            body(i)
            return carry

        lax.fori_loop(lo, hi, step, 0)

    def ranked(index, n, odd):
        moved = jnp.where(index == 0, n - 2, jnp.where(index == n - 1, n - 1, index - 1))
        return jnp.where(odd, moved, index)

    def unranked(rank, n, odd):
        moved = jnp.where(rank == n - 2, 0, jnp.where(rank == n - 1, n - 1, rank + 1))
        return jnp.where(odd, moved, rank)

    def folded(index):
        return jnp.where(index < half, index, n_x - 1 - index + half)

    z_odd, x_odd, c_odd = (me == 0) & (core == 0), (z == 0) & (core == 0), (z == 0) & (me == 0)
    z_rank = ranked(z, n_z, z_odd)
    x_rank = jnp.where(x_odd, lax.rem(folded(me) + n_x - 1, n_x), folded(me))
    c_rank = jnp.where(c_odd, 1 - core, core)

    def z_of(rank):
        return unranked(rank, n_z, z_odd)

    def x_of(rank):
        return folded(jnp.where(x_odd, lax.rem(rank + 1, n_x), rank))

    barrier = pltpu.get_barrier_semaphore()
    each(z_rank + 1, n_z, lambda r: signal(barrier, at_chip(z_of(r))))
    each(x_rank + 1, n_x, lambda r: signal(barrier, {"tp": x_of(r)}))

    @pl.when(c_rank == 0)
    def _():
        signal(barrier, partner)

    smalls = (
        (tokens_hbm, tokens_ref),
        (group_hbm, group_ref),
        (gain_hbm, gain_ref),
        (member_hbm, member_ref),
        (prob_hbm, prob_ref),
        (score_hbm, score_ref),
        (final_hbm, final_ref),
    )
    fetched = [pltpu.make_async_copy(src, dst, in_sem.at[i]) for i, (src, dst) in enumerate(smalls)]
    for fetch in fetched:
        fetch.start()
    loads = []
    for o in range(n_x):
        part = pl.ds(o * cols, cols)
        loads.append(pltpu.make_async_copy(wg_ref.at[0, :, part], wgu.at[o, :, pl.ds(0, cols)], w_sem.at[0]))
        loads.append(pltpu.make_async_copy(wu_ref.at[0, :, part], wgu.at[o, :, pl.ds(cols, cols)], w_sem.at[0]))
    loads.append(pltpu.make_async_copy(wd_ref.at[0], wdn, w_sem.at[1]))
    for load in loads:
        load.start()

    for fetch in fetched:
        fetch.wait()
    values = tokens_ref[...].astype(F32)
    scaled = (values * gain_ref[...]).astype(BF16)
    group_row = group_ref[...]
    chosen = (iota((8, tok), 0) == jnp.broadcast_to(group_row, (8, tok))).astype(F32)
    earlier = (iota((tok, tok), 0) < iota((tok, tok), 1)).astype(F32)
    rank = jnp.sum(dot(chosen, earlier) * chosen, axis=0, keepdims=True)
    slot_row = group_row.astype(F32) * cap + rank
    picker = (iota((tok, tok), 0).astype(F32) == jnp.broadcast_to(slot_row, (tok, tok))).astype(BF16)
    sorted_buf[...] = dot(picker, scaled).astype(BF16)
    square = jnp.sum(values * values, axis=1, keepdims=True)
    sq_buf[pl.ds(me, 1)] = row_of(square, 128).reshape(1, 1, 128)
    rows_mine[block(z), :] = sorted_buf[block(lax.div(z, per_chips)), :]

    def send_rows(k):
        send(sorted_buf.at[block(lax.div(k, per_chips))], rows_mine.at[block(z)], z_send.at[0], z_recv.at[z], at_chip(k))

    def send_meta(k):
        send(meta_src.at[block(lax.div(k, per_chips))], meta_mine.at[block(z)], z_send.at[1], m_recv.at[z], at_chip(k))

    with jax.named_scope("meet"):
        expected = z_rank + x_rank + c_rank

        @pl.when(expected > 0)
        def _():
            pl.semaphore_wait(barrier, expected)

        each(0, z_rank, lambda r: signal(here_z.at[z], at_chip(z_of(r))))
        each(0, x_rank, lambda r: signal(here_x.at[me], {"tp": x_of(r)}))

        @pl.when(c_rank == 1)
        def _():
            signal(here_c, partner)

    def greet(r):
        k = z_of(r)
        pl.semaphore_wait(here_z.at[k], 1)
        send_rows(k)

    with jax.named_scope("greet"):
        each(0, z_rank, lambda r: send_rows(z_of(r)))
        each(z_rank + 1, n_z, greet)

    def send_square(r):
        send(sq_buf.at[me], sq_buf.at[me], sq_send.at[0], sq_recv.at[0], {"tp": x_of(r)})

    def greet_x(r):
        pl.semaphore_wait(here_x.at[x_of(r)], 1)
        send_square(r)

    with jax.named_scope("greet_x"):
        each(0, x_rank, send_square)
        each(x_rank + 1, n_x, greet_x)

        @pl.when(c_rank == 0)
        def _():
            pl.semaphore_wait(here_c, 1)

    def await_blocks(c, ref, sems):
        for k in range(bases[c], bases[c] + CHUNKS[c]):

            @pl.when(z != k)
            def _(k=k):
                await_bytes(ref.at[pl.ds(k * cap, cap)], sems.at[k])

    def take(c):
        await_blocks(c, rows_mine, z_recv)
        send(rows_mine.at[span(c)], rows_other.at[span(c)], fwd_send.at[c], fwd_recv.at[c], partner)

    def make_meta():
        await_bytes(sq_buf.at[pl.ds(0, n_x - 1)], sq_recv.at[0])
        total = jnp.sum(sq_buf[...], axis=0)[:, :tok]
        factor = lax.rsqrt(total / width + EPS)
        score = jnp.exp(score_ref[...])
        weight = prob_ref[...] * score / jnp.sum(score, axis=0, keepdims=True)
        member = iota((8, tok), 0)
        dense = jnp.zeros((8, tok), F32)
        for k in range(member_ref.shape[0]):
            dense = jnp.where(member == member_ref[k : k + 1, :], weight[k : k + 1, :], dense)
        parts = split3(dense)
        factors = split3(factor)
        spread = jnp.zeros((8, tok), F32)
        for k in range(3):
            spread = jnp.where(member == k, factors[k], spread)
        packed = jnp.concatenate([*parts, spread, jnp.zeros((96, tok), F32)], axis=0)
        meta_src[...] = lax.dot_general(
            picker, packed.astype(BF16), (((1,), (1,)), ((), ())), preferred_element_type=F32
        ).astype(BF16)
        meta_mine[block(z), :] = meta_src[block(lax.div(z, per_chips)), :]
        each(0, z_rank, lambda r: send_meta(z_of(r)))
        each(z_rank + 1, n_z, lambda r: send_meta(z_of(r)))

    def pass_meta(c):
        await_blocks(c, meta_mine, m_recv)
        send(meta_mine.at[span(c)], meta_other.at[span(c)], mfwd_send.at[c], mfwd_recv.at[c], partner)

    gate_cols, up_cols = pl.ds(0, cols), pl.ds(cols, cols)

    def partial(c, owner):
        both = jnp.concatenate([rows_mine[span(c), :], rows_other[span(c), :]], axis=0)
        return dot(both, wgu[owner])

    def reduce_ref(buf, c, s, d):
        used = pl.ds(0, 2 * n_mine(c))
        if s > 0:
            return buf.at[c, s, d, used]
        return buf.at[c, s, d, used, up_cols if d == 0 else gate_cols]

    def await_reduce(c, s, d):
        await_bytes(reduce_ref(rs_recv, c, s, d), rs_rsem.at[c, s, d])

    def reduce_send(c, s, d):
        send(
            reduce_ref(rs_send, c, s, d),
            reduce_ref(rs_recv, c, s, d),
            rs_ssem.at[c, s, d],
            rs_rsem.at[c, s, d],
            right if d == 0 else left,
        )

    def reduce_step(c, s):
        n = 2 * n_mine(c)
        if s == 0:
            both = partial(c, x_index(half)).astype(BF16)
            rs_send[c, 0, 0, :n, cols:] = both[:, cols:]
            rs_send[c, 0, 1, :n, :cols] = both[:, :cols]
            reduce_send(c, 0, 0)
            reduce_send(c, 0, 1)
            return
        for d, sign in enumerate((1, -1)):
            mine = partial(c, x_index(sign * (half - s)))
            await_reduce(c, s - 1, d)
            if s == 1:
                lo = d * cols
                alone = slice(lo, lo + cols)
                other = slice(cols - lo, 2 * cols - lo)
                rs_send[c, s, d, :n, alone] = mine[:, alone].astype(BF16)
                rs_send[c, s, d, :n, other] = (mine[:, other] + rs_recv[c, s - 1, d, :n, other].astype(F32)).astype(BF16)
            else:
                rs_send[c, s, d, :n] = (mine + rs_recv[c, s - 1, d, :n].astype(F32)).astype(BF16)
            reduce_send(c, s, d)

    def gather_ref(c, s, d, owner):
        if s < half - 1:
            return hid.at[c, owner, pl.ds(0, 2 * n_mine(c))]
        return hid.at[c, owner, pl.ds(d * n_mine(c), n_mine(c))]

    def gather_all(c):
        for r in range(1, n_x):
            block_me = hid.at[c, me, pl.ds(0, 2 * n_mine(c))]
            send(block_me, block_me, ag_ssem.at[c, 0, 0], ag_rsem.at[c, 0, 0], {"tp": x_index(r)})

    def gather_send(c, s):
        for d, sign in enumerate((1, -1)):
            ref = gather_ref(c, s, d, x_index(-sign * s))
            send(ref, ref, ag_ssem.at[c, s, d], ag_rsem.at[c, s, d], right if d == 0 else left)

    def gather_wait(c, s):
        for d, sign in enumerate((1, -1)):
            await_bytes(gather_ref(c, s, d, x_index(-sign * (s + 1))), ag_rsem.at[c, s, d])

    def info(c):
        return jnp.concatenate([meta_mine[span(c), :], meta_other[span(c), :]], axis=0).astype(F32)

    def activate(c):
        n = 2 * n_mine(c)
        total = partial(c, me)
        await_bytes(meta_other.at[span(c)], mfwd_recv.at[c])
        lane = iota((n, 128), 1)
        factor = jnp.sum(jnp.where(lax.div(lane, 8) == 3, info(c), 0.0), axis=1, keepdims=True)
        for d in range(2):
            await_reduce(c, half - 1, d)
            total = total + rs_recv[c, half - 1, d, :n].astype(F32)
        total = total * factor
        gate, up = total[:, :cols], total[:, cols:]
        hid[c, me, :n] = (gate / (1.0 + jnp.exp(-gate)) * up).astype(BF16)
        if c in DIRECT:
            gather_all(c)
        else:
            gather_send(c, 0)

    def all_others(c):
        return hid.at[c, pl.ds(0, n_x - 1), pl.ds(0, 2 * n_mine(c))]

    def produce(c):
        n = 2 * n_mine(c)
        if c in DIRECT:
            await_bytes(all_others(c), ag_rsem.at[c, 0, 0])
        else:
            gather_wait(c, half - 1)
        hidden = jnp.concatenate([hid[c, o, :n] for o in range(n_x)], axis=1)
        made = dot(hidden, wdn[...])
        lane = iota((n, 128), 1)
        member = 2 * lax.rem(z, per_chips) + core
        named = (lax.rem(lane, 8) == member) & (lane < 24)
        weight = jnp.sum(jnp.where(named, info(c), 0.0), axis=1, keepdims=True)
        made = made.astype(BF16).astype(F32) * weight
        pair_send[span(c), :] = made[n_mine(c) :].astype(BF16)
        send(pair_send.at[span(c)], pair_recv.at[span(c)], pair_ssem.at[c], pair_rsem.at[c], partner)
        kept[span(c), :] = made[: n_mine(c)]

    def give_back(c):
        await_bytes(pair_recv.at[span(c)], pair_rsem.at[c])
        ret_send[span(c), :] = (kept[span(c), :] + pair_recv[span(c), :].astype(F32)).astype(BF16)
        for k in range(bases[c], bases[c] + CHUNKS[c]):

            @pl.when(z == k)
            def _(k=k):
                ret_recv[block(k), :] = ret_send[block(k), :]

            @pl.when(z != k)
            def _(k=k):
                send(ret_send.at[block(k)], ret_recv.at[block(z)], z_send.at[2], r_recv.at[z], at_chip(k))

    def gather_returned():
        for k in range(n_z):

            @pl.when(z != k)
            def _(k=k):
                await_bytes(ret_recv.at[block(k)], r_recv.at[k])

        row = iota((n_z * cap, tok), 0)
        slots = lax.div(row, per_chips * cap) * cap + lax.rem(row, cap)
        unpick = (slots.astype(F32) == jnp.broadcast_to(slot_row, row.shape)).astype(BF16)
        moe = lax.dot_general(unpick, ret_recv[...], (((0,), (0,)), ((), ())), preferred_element_type=F32)
        summed = tokens_ref[...].astype(F32) + moe
        summed_buf[...] = summed
        total = jnp.sum(summed * summed, axis=1, keepdims=True)
        sq2_buf[pl.ds(me, 1)] = row_of(total, 128).reshape(1, 1, 128)

        def send_total(r):
            send(sq2_buf.at[me], sq2_buf.at[me], sq_send.at[1], sq_recv.at[1], {"tp": r})

        each(0, me, send_total)
        each(me + 1, n_x, send_total)

    def write_out():
        await_bytes(sq2_buf.at[pl.ds(0, n_x - 1)], sq_recv.at[1])
        total = column_of(jnp.sum(sq2_buf[...], axis=0), tok)
        out_ref[...] = (summed_buf[...] * lax.rsqrt(total / width + EPS) * final_ref[...]).astype(BF16)

    def stage(c, k):
        if k == 0:
            await_bytes(rows_other.at[span(c)], fwd_recv.at[c])
            reduce_step(c, 0)
        elif k < half:
            reduce_step(c, k)
            if k == half - 2:
                pass_meta(c)
        elif k == half:
            activate(c)
        elif c in DIRECT:
            (produce if k == half + 1 else give_back)(c)
        elif k < 2 * half:
            gather_wait(c, k - half - 1)
            gather_send(c, k - half)
        elif k == 2 * half:
            produce(c)
        else:
            give_back(c)

    ends = [half + 2 if c in DIRECT else 2 * half + 1 for c in range(n_chunks)]
    total_steps = max(START[c] + ends[c] for c in range(n_chunks)) + 1
    for c in ORDER:
        if START[c] == 0:
            with jax.named_scope(f"take#c={c}"):
                take(c)
    with jax.named_scope("weights"):
        await_bytes(wgu, w_sem.at[0])
        await_bytes(wdn, w_sem.at[1])
    for t in range(total_steps):
        for c in ORDER:
            k = t - START[c]
            if 0 <= k <= ends[c]:
                with jax.named_scope(f"stage#c={c}#k={k}"):
                    stage(c, k)
        if t == 1:
            with jax.named_scope("make_meta"):
                make_meta()
        for c in ORDER:
            if t == START[c] - 1:
                with jax.named_scope(f"take#c={c}"):
                    take(c)
    with jax.named_scope("returned"):
        gather_returned()
    with jax.named_scope("write"):
        write_out()

    n_remote = cap * (n_z - 1)
    flat = wdn.at[pl.ds(0, n_remote)]
    await_bytes(flat, z_send.at[0])
    await_bytes(wdn.at[pl.ds(0, n_remote), pl.ds(0, 128)], z_send.at[1])
    await_bytes(flat, z_send.at[2])
    await_bytes(sq_buf.at[pl.ds(0, n_x - 1)], sq_send.at[0])
    await_bytes(sq_buf.at[pl.ds(0, n_x - 1)], sq_send.at[1])
    for c in range(n_chunks):
        await_bytes(rows_mine.at[span(c)], fwd_send.at[c])
        await_bytes(meta_mine.at[span(c)], mfwd_send.at[c])
        await_bytes(pair_recv.at[span(c)], pair_ssem.at[c])
        if c in DIRECT:
            await_bytes(all_others(c), ag_ssem.at[c, 0, 0])
        for s in range(half):
            for d in range(2):
                await_bytes(reduce_ref(rs_send, c, s, d), rs_ssem.at[c, s, d])
                if c not in DIRECT:
                    await_bytes(gather_ref(c, s, d, me), ag_ssem.at[c, s, d])


def local(tokens, group_choice, member_choice, group_prob, member_score, norm_gain, w_gate, w_up, w_down, final_gain):
    n_z, n_x = lax.axis_size("ep") // 2, lax.axis_size("tp")
    groups = max(2, 2 * n_z // 8)
    tok, dl = tokens.shape
    top = member_choice.shape[1]
    ff = w_gate.shape[2]
    cap = tok // groups
    cols = ff // n_x
    n_chunks = len(CHUNKS)
    n_rows = 2 * cap * max(CHUNKS)
    n_all = n_z * cap
    half = n_x // 2
    dma = pltpu.SemaphoreType.DMA
    vmem = pl.BlockSpec(memory_space=pltpu.VMEM)
    hbm = pl.BlockSpec(memory_space=pl.ANY)
    return pl.pallas_call(
        functools.partial(kernel, (n_z, n_x, groups, dl * n_x)),
        out_shape=jax.ShapeDtypeStruct((tok, dl), BF16),
        in_specs=[hbm] * 10,
        out_specs=vmem,
        scratch_shapes=[
            pltpu.VMEM((tok, dl), BF16),
            pltpu.VMEM((1, tok), jnp.int32),
            pltpu.VMEM((top, tok), jnp.int32),
            pltpu.VMEM((1, tok), F32),
            pltpu.VMEM((top, tok), F32),
            pltpu.VMEM((1, dl), F32),
            pltpu.VMEM((1, dl), F32),
            dma((7,)),
            pltpu.VMEM((n_x, dl, 2 * cols), BF16),
            pltpu.VMEM((ff, dl), BF16),
            pltpu.VMEM((tok, dl), BF16),
            pltpu.VMEM((tok, 128), BF16),
            pltpu.VMEM((n_all, dl), BF16),
            pltpu.VMEM((n_all, dl), BF16),
            pltpu.VMEM((n_all, 128), BF16),
            pltpu.VMEM((n_all, 128), BF16),
            pltpu.VMEM((n_x, 1, 128), F32),
            pltpu.VMEM((n_x, 1, 128), F32),
            pltpu.VMEM((n_chunks, half, 2, n_rows, 2 * cols), BF16),
            pltpu.VMEM((n_chunks, half, 2, n_rows, 2 * cols), BF16),
            pltpu.VMEM((n_chunks, n_x, n_rows, cols), BF16),
            pltpu.VMEM((n_all, dl), F32),
            pltpu.VMEM((n_all, dl), BF16),
            pltpu.VMEM((n_all, dl), BF16),
            pltpu.VMEM((n_all, dl), BF16),
            pltpu.VMEM((n_all, dl), BF16),
            pltpu.VMEM((tok, dl), F32),
            dma((2,)),
            dma((3,)),
            dma((n_z,)),
            dma((n_z,)),
            dma((n_z,)),
            dma((n_chunks,)),
            dma((n_chunks,)),
            dma((n_chunks,)),
            dma((n_chunks,)),
            dma((2,)),
            dma((2,)),
            dma((n_chunks, half, 2)),
            dma((n_chunks, half, 2)),
            dma((n_chunks, half, 2)),
            dma((n_chunks, half, 2)),
            dma((n_chunks,)),
            dma((n_chunks,)),
            pltpu.SemaphoreType.REGULAR((n_z,)),
            pltpu.SemaphoreType.REGULAR((n_x,)),
            pltpu.SemaphoreType.REGULAR,
        ],
        compiler_params=pltpu.CompilerParams(
            collective_id=0, has_side_effects=True, vmem_limit_bytes=67043328
        ),
    )(
        tokens,
        group_choice.reshape(1, tok),
        member_choice.T,
        group_prob.reshape(1, tok),
        member_score.T,
        norm_gain.reshape(1, dl),
        final_gain.reshape(1, dl),
        w_gate,
        w_up,
        w_down,
    )


def solution(mesh):
    rows = ("grp", "ep")
    placed = (
        P(rows, "tp"),
        P(rows),
        P(rows, None),
        P(rows),
        P(rows, None),
        P("tp"),
        P("ep", "tp", None),
        P("ep", "tp", None),
        P("ep", None, "tp"),
        P("tp"),
    )
    return jax.shard_map(local, mesh=mesh, in_specs=placed, out_specs=P(rows, "tp"), check_vma=False)
```
